32 devices in a mesh: sp: 8 (over z, x), tp: 4 (over y, core).
Axes of the slice: x: 2, y: 2, z: 4, core: 2. Of those that a mesh axis runs over, the one named last changes fastest.
Arguments:
- cotangent: bfloat16 [2048, 2048], P('sp'), may hold values from -6 to 6
- route_ids: int32 [2048, 2], P('sp'), may hold values from 0 to 7, all different within a row; in each aligned block of 256 rows (0 to 255, 256 to 511, ...) at most 128 rows name the same one
- route_weights: float32 [2048, 2], P('sp'), may hold values from 0.2 to 1
- expert_inputs: bfloat16 [8, 1024, 2048], P('sp'), may hold values from -6 to 6
- gate_weight: bfloat16 [8, 2048, 1024], P('sp', None, 'tp'), may hold values from -0.125 to 0.125
- up_weight: bfloat16 [8, 2048, 1024], P('sp', None, 'tp'), may hold values from -0.125 to 0.125
- down_weight: bfloat16 [8, 1024, 2048], P('sp', 'tp'), may hold values from -0.1875 to 0.1875
- out_weight: bfloat16 [2048, 512], P(None, 'tp'), may hold values from -0.25 to 0.25
- gate_in: bfloat16 [2048, 512], P('sp', 'tp'), may hold values from -6 to 6
- conv_sum: bfloat16 [2048, 512], P('sp', 'tp'), may hold values from -6 to 6
- conv_c: bfloat16 [2048, 512], P('sp', 'tp'), may hold values from -6 to 6
- conv_v: bfloat16 [2048, 512], P('sp', 'tp'), may hold values from -6 to 6
- conv_taps: float32 [3, 512], P(None, 'tp'), may hold values from -3 to 3
Outputs:
- grad_input: bfloat16 [2048, 2048], P('sp', 'tp')
- grad_gate: bfloat16 [8, 2048, 1024], P('sp', None, 'tp')
- grad_up: bfloat16 [8, 2048, 1024], P('sp', None, 'tp')
- grad_down: bfloat16 [8, 1024, 2048], P('sp', 'tp')
- grad_out_weight: float32 [2048, 512], P('sp', 'tp')
- grad_gate_in: bfloat16 [2048, 512], P('sp', 'tp')
- grad_conv_c: bfloat16 [2048, 512], P('sp', 'tp')
- grad_conv_v: bfloat16 [2048, 512], P('sp', 'tp')
The draws below stay inside these ranges and needn't reach their ends.
Inputs may be any that keep to these rules, and one draw needn't show every extreme that they name: `route_ids`: the 2 experts of a token differ. Among the 256 tokens of one index of sp no expert is named more than 128 times, and in every draw some expert is named exactly 128 times by the tokens of some index of sp.
All inputs are finite; a program needn't handle non-finite values.
Results may differ from the reference program's by a relative error of at most 0.012.
Values may be sent and summed in bfloat16 or wider, within the bound.
A program may use at most 128 MiB of HBM per device.

```python
import math
import jax
import jax.numpy as jnp
import numpy as np
from jax import lax

D = 2048
F = 1024
W = 512
TOP = 2
TAPS = 3
TOK_DEV = 256
EXPERTS = 8
CAP = 128
TOKENS = 2048
N_SP = 8
N_TP = 4


def spiked(result, rng, source, target, parts, factor):
    owner, partner = [(jnp.arange(result.shape[dim]) // (result.shape[dim] // parts)).reshape([-1 if axis == dim else 1 for axis in range(result.ndim)]) for dim in (source, target)]
    chosen = jax.random.permutation(rng, parts)[partner]
    strong = (owner == chosen) | (owner == (partner + parts // 2) % parts)
    return jnp.where(strong, factor * result, result)


def shard_levels(stream_key, extent, cuts, smallest, largest):
    def one(position, blocks):
        heights = jax.random.uniform(jax.random.fold_in(jax.random.fold_in(stream_key, 6), position), (blocks,), jnp.float32, smallest / len(cuts), largest / len(cuts))
        return jnp.repeat(jnp.exp(heights), extent[position] // blocks).reshape((-1,) + (1,) * (len(extent) - position - 1))

    gain = one(*cuts[0])
    for cut in cuts[1:]:
        gain = gain * one(*cut)
    return gain


def deal_out(own_key, own, number, rows, number_of, top, most, lean):
    order = jax.random.permutation(own_key, number_of)
    packed, ordinary = shares(number_of, rows * top, most, lean, True), shares(number_of, rows * top, most, lean, False)
    places = jnp.arange(number_of)

    def named(sizes, offset_by):
        used = int((sizes > 0).sum())
        fixed = max(1, used // 4)
        passed = fixed + (places - fixed + offset_by * (used - fixed)) % max(1, number_of - fixed)
        return jnp.zeros((number_of,), jnp.int32).at[order[jnp.where(places < fixed, places, passed)]].set(jnp.asarray(sizes, jnp.int32))

    sizes = jnp.where(number % 4 == 0, named(packed, number // 4), named(ordinary, number - number // 4 - 1))
    mixed = jax.random.permutation(jax.random.fold_in(own, 3), number_of)
    giver, receiver = mixed[0:number_of // 2 * 2:2], mixed[1:number_of // 2 * 2:2]
    room = jnp.minimum(sizes[giver] - 1, most - sizes[receiver]) // 2
    room = jnp.where((giver == order[0]) | (receiver == order[0]) | (sizes[receiver] == 0), 0, jnp.maximum(room, 0))
    passed = jax.random.randint(jax.random.fold_in(own, 4), (number_of // 2,), 0, 1 << 20) % (room + 1)
    sizes = sizes.at[giver].add(-passed).at[receiver].add(passed)
    labels = jnp.searchsorted(jnp.cumsum(sizes), jnp.arange(rows * top), side="right").astype(jnp.int32)
    table = labels.reshape(top, rows).T
    table = table[jax.random.permutation(jax.random.fold_in(own, 1), rows)]
    offset_by = jax.random.randint(jax.random.fold_in(own, 2), (rows, 1), 0, top)
    return jnp.take_along_axis(table, (jnp.arange(top)[None, :] + offset_by) % top, axis=1)


def shares(amount, total, bound, slope, full):
    loads = [(1 << 20) // math.isqrt(grade ** slope) + 1 for grade in range(1, amount + 1)]
    largest = bound if full else min(bound, max(-(-total // amount), total * loads[0] // sum(loads)))
    least = 1 if total - largest >= amount - 1 else 0
    counts, spare = [largest] + [least] * (amount - 1), total - largest - least * (amount - 1)
    while spare > 0:
        free = [i for i in range(1, amount) if counts[i] < largest] or [i for i in range(1, amount) if counts[i] < bound]
        mass, remaining = sum([loads[i] for i in free]), spare
        for i in free:
            more = min(bound - counts[i], max(1, remaining * loads[i] // mass), spare)
            counts[i] = counts[i] + more
            spare = spare - more
    return np.array(counts)


def scatter_about(stream_key, extent, scale, bound, split=(), kind=jnp.bfloat16):
    result = jax.random.normal(stream_key, extent, jnp.float32) * scale
    if len(split) > 0:
        result = shard_levels(stream_key, extent, split, -0.22, 0.18) * result
    return jnp.clip(result, min=-bound, max=bound).astype(kind)


def gaussian_with(own_key, extent, scale, limit, shards, heavy, held_as=jnp.bfloat16):
    array = scale * jax.random.normal(own_key, extent, jnp.float32)
    if shards:
        array = array * shard_levels(own_key, extent, shards, -0.22, 0.18)
    return jnp.clip(spiked(array, jax.random.fold_in(own_key, 3), *heavy), -limit, limit).astype(held_as)


def setup_inputs(seed: int = 0) -> dict:
    key_list = jax.random.split(jax.random.key(seed), 14)
    cotangent = gaussian_with(key_list[0], (TOKENS, D), 1.0, 6.0, ((0, 8),), (0, 1, 8, 2.0))
    route_ids_keys = jax.random.split(jax.random.fold_in(key_list[1], 1), TOKENS // TOK_DEV)
    route_ids_turns = jax.random.permutation(jax.random.fold_in(key_list[1], 3), TOKENS // TOK_DEV)
    route_ids = jax.vmap(lambda own, number: deal_out(jax.random.fold_in(key_list[1], 2), own, number, TOK_DEV, EXPERTS, TOP, CAP, 1))(route_ids_keys, route_ids_turns).reshape((TOKENS, TOP))
    route_weights = jnp.clip(0.2 + 0.8 * jax.random.uniform(key_list[2], (TOKENS, TOP), jnp.float32) ** shard_levels(key_list[2], (TOKENS, TOP), ((0, 8),), -0.2, 0.2), 0.2, 1.0)
    expert_inputs = scatter_about(key_list[3], (EXPERTS, N_SP * CAP, D), 1.0, 6.0, ((0, 8),))
    gate_weight = scatter_about(key_list[4], (EXPERTS, D, F), D ** -0.5, 0.125, ((0, 8), (2, 4)))
    up_weight = scatter_about(key_list[5], (EXPERTS, D, F), D ** -0.5, 0.125, ((0, 8), (2, 4)))
    down_weight = scatter_about(key_list[6], (EXPERTS, F, D), F ** -0.5, 0.1875, ((0, 8), (1, 4)))
    out_weight = scatter_about(key_list[7], (D, W), W ** -0.5, 0.25, ((1, 4),))
    gate_in = scatter_about(key_list[8], (TOKENS, W), 1.0, 6.0, ((0, 8), (1, 4)))
    conv_sum = scatter_about(key_list[9], (TOKENS, W), 1.0, 6.0, ((0, 8), (1, 4)))
    conv_c = scatter_about(key_list[10], (TOKENS, W), 1.0, 6.0, ((0, 8), (1, 4)))
    conv_v = scatter_about(key_list[11], (TOKENS, W), 1.0, 6.0, ((0, 8), (1, 4)))
    conv_taps = scatter_about(key_list[12], (TAPS, W), 0.6, 3.0, ((1, 4),), jnp.float32)
    return dict(cotangent=cotangent, route_ids=route_ids, route_weights=route_weights, expert_inputs=expert_inputs, gate_weight=gate_weight, up_weight=up_weight, down_weight=down_weight, out_weight=out_weight, gate_in=gate_in, conv_sum=conv_sum, conv_c=conv_c, conv_v=conv_v, conv_taps=conv_taps)


def reference(cotangent, route_ids, route_weights, expert_inputs, gate_weight, up_weight, down_weight, out_weight, gate_in, conv_sum, conv_c, conv_v, conv_taps):
    experts = gate_weight.shape[0]
    pair_ids = route_ids.reshape(N_SP, TOK_DEV * TOP)
    onehot = (pair_ids[:, :, None] == jnp.arange(experts, dtype=jnp.int32)[None, None, :]).astype(jnp.int32)
    before = jnp.cumsum(onehot, axis=1) - onehot
    ranked = jnp.sum(before * onehot, axis=2)
    source = jnp.arange(N_SP, dtype=jnp.int32)[:, None]
    slot_row = (source * CAP + ranked).reshape(-1).astype(jnp.int32)
    target = pair_ids.reshape(-1).astype(jnp.int32)
    weighted = (route_weights[:, :, None] * cotangent.astype(jnp.float32)[:, None, :]).astype(jnp.bfloat16).reshape(-1, D)
    routed = jnp.zeros((experts, N_SP * CAP, D), jnp.bfloat16).at[target, slot_row].set(weighted)
    quarter = F // N_TP

    def expert_step(expert_items):
        stored, grad_rows, w_gate, w_up, w_down = expert_items
        pre_gate = jnp.dot(stored, w_gate, preferred_element_type=jnp.float32)
        pre_up = jnp.dot(stored, w_up, preferred_element_type=jnp.float32)
        gate_sig = jax.nn.sigmoid(pre_gate)
        swish_gate = pre_gate * gate_sig
        hidden = (swish_gate * pre_up).astype(jnp.bfloat16)
        grad_hidden = jnp.dot(grad_rows, w_down.T, preferred_element_type=jnp.float32)
        grad_pregate = (grad_hidden * pre_up * gate_sig * (1.0 + pre_gate * (1.0 - gate_sig))).astype(jnp.bfloat16)
        grad_preup = (grad_hidden * swish_gate).astype(jnp.bfloat16)
        grad_down = jnp.dot(hidden.T, grad_rows, preferred_element_type=jnp.float32).astype(jnp.bfloat16)
        grad_gate = jnp.dot(stored.T, grad_pregate, preferred_element_type=jnp.float32).astype(jnp.bfloat16)
        grad_up = jnp.dot(stored.T, grad_preup, preferred_element_type=jnp.float32).astype(jnp.bfloat16)
        total = jnp.zeros((stored.shape[0], D), jnp.float32)
        for part_index in range(N_TP):
            low = part_index * quarter
            high = low + quarter
            part = jnp.dot(grad_pregate[:, low:high], w_gate[:, low:high].T, preferred_element_type=jnp.float32)
            part = part + jnp.dot(grad_preup[:, low:high], w_up[:, low:high].T, preferred_element_type=jnp.float32)
            total = total + lax.optimization_barrier(part.astype(jnp.bfloat16)).astype(jnp.float32)
        return grad_gate, grad_up, grad_down, total.astype(jnp.bfloat16)

    grad_gate, grad_up, grad_down, grad_x = lax.map(expert_step, (expert_inputs, routed, gate_weight, up_weight, down_weight))
    returned = grad_x[target, slot_row].astype(jnp.float32).reshape(TOKENS, TOP, D)
    grad_input = (cotangent.astype(jnp.float32) + jnp.sum(returned, axis=1)).astype(jnp.bfloat16)
    mixed_rows = (gate_in.astype(jnp.float32) * conv_sum.astype(jnp.float32)).astype(jnp.bfloat16)
    grad_mixed = jnp.dot(grad_input, out_weight, preferred_element_type=jnp.float32)
    grad_out_weight = jnp.dot(grad_input.T, mixed_rows, preferred_element_type=jnp.float32)
    grad_gate_in = (grad_mixed * conv_sum.astype(jnp.float32)).astype(jnp.bfloat16)
    grad_sum = grad_mixed * gate_in.astype(jnp.float32)
    extended = jnp.concatenate([grad_sum, jnp.zeros((2, grad_sum.shape[1]), jnp.float32)], axis=0)
    grad_prod = conv_taps[0] * extended[2:] + conv_taps[1] * extended[1:-1] + conv_taps[2] * extended[:-2]
    grad_conv_c = (grad_prod * conv_v.astype(jnp.float32)).astype(jnp.bfloat16)
    grad_conv_v = (grad_prod * conv_c.astype(jnp.float32)).astype(jnp.bfloat16)
    return (grad_input, grad_gate, grad_up, grad_down, grad_out_weight, grad_gate_in, grad_conv_c, grad_conv_v)
```

```python
import functools

import jax
import jax.numpy as jnp
from jax import lax
from jax.experimental import pallas as pl
from jax.experimental.pallas import tpu as pltpu
from jax.sharding import PartitionSpec as P

F32 = jnp.float32
BF16 = jnp.bfloat16
NT = (((1,), (1,)), ((), ()))
TN = (((0,), (0,)), ((), ()))


def mm(a, b, dims=(((1,), (0,)), ((), ()))):
    return lax.dot_general(a, b, dims, preferred_element_type=F32)


def kernel(
    n,
    tp,
    ids_ref,
    wts_ref,
    cot_ref,
    x_hbm,
    wg_hbm,
    wu_hbm,
    wd_hbm,
    ow_ref,
    gin_ref,
    csum_ref,
    cc_ref,
    cv_ref,
    taps_ref,
    gi_hbm,
    gg_hbm,
    gu_hbm,
    gd_hbm,
    gow_out,
    ggi_out,
    gcc_out,
    gcv_out,
    x_v,
    wg_v,
    wu_v,
    wd_v,
    sel_v,
    sent_v,
    pair_v,
    routed_v,
    pre_g,
    pre_u,
    hid_v,
    gpg_v,
    gpu_v,
    part_v,
    core_v,
    ysend_v,
    yrecv_v,
    back_v,
    ret_v,
    mid_v,
    term_v,
    terms_v,
    ext_v,
    halo_v,
    gg_v,
    gu_v,
    gd_v,
    load_sem,
    save_sem,
    out_s,
    out_r,
    pair_s,
    pair_r,
    agy_s,
    agy_r,
    agd_s,
    agd_r,
    fwd_s,
    fwd_r,
    core_s,
    core_r,
    y_s,
    y_r,
    ret_s,
    ret_r,
    mid_s,
    mid_r,
    term_s,
    term_r,
    halo_s,
    halo_r,
):
    me = lax.axis_index("sp")
    q = lax.axis_index("tp")
    qd = q + 1 - 2 * (q % 2)
    qy = (q + tp // 2) % tp
    qdy = (qd + tp // 2) % tp
    tokens, width = cot_ref.shape
    slots = x_v.shape[0]
    cap = slots // n
    dq = width // tp
    du = dq // 2
    top = ids_ref.shape[0]

    loads = [
        pltpu.make_async_copy(src.at[0], dst, load_sem.at[i])
        for i, (src, dst) in enumerate(
            ((x_hbm, x_v), (wg_hbm, wg_v), (wu_hbm, wu_v), (wd_hbm, wd_v))
        )
    ]
    for load in loads:
        load.start()

    barrier = pltpu.get_barrier_semaphore()

    def greet(i, carry):
        pl.semaphore_signal(
            barrier, inc=1, device_id=((me + i) % n, q), device_id_type=pl.DeviceIdType.MESH
        )
        return carry

    lax.fori_loop(1, n, greet, 0)
    for other in (qd, qy):
        pl.semaphore_signal(
            barrier, inc=1, device_id=(me, other), device_id_type=pl.DeviceIdType.MESH
        )

    def rows(block):
        return pl.ds(pl.multiple_of(block * cap, cap), cap)

    def unit(part, side):
        return pl.ds(pl.multiple_of((part + side * tp) * du, du), du)

    def gathered(ref, part):
        return jnp.concatenate([ref[:, unit(part, 0)], ref[:, unit(part, 1)]], axis=1)

    def remote(src, dst, ssem, rsem, sp_id, tp_id):
        return pltpu.make_async_remote_copy(
            src_ref=src,
            dst_ref=dst,
            send_sem=ssem,
            recv_sem=rsem,
            device_id=(sp_id, tp_id),
            device_id_type=pl.DeviceIdType.MESH,
        )

    half = n // 2
    pairs = half // 2
    side, low = me // half, me % half
    pair, member = low // 2, low % 2

    twin = n - 1

    def step(p):
        far = (p == 1) | ((p >= 3) & (p < half + 2))
        across = jnp.where(far, 1, 0)
        late = jnp.where(p < 3, p, jnp.where(p == twin, 1, p - half + 1))
        turn = jnp.where(far, jnp.where(p == 1, 0, p - 2), late)
        return (side + across) % 2 * half, turn // 2, turn % 2

    def to(i):
        base, hop, swap = step(i)
        return base + (pair + hop) % pairs * 2 + (member + swap) % 2

    def source(i):
        base, hop, swap = step(i)
        return base + (pair - hop + pairs) % pairs * 2 + (member + swap) % 2

    def c_out(i):
        return remote(
            sent_v.at[rows(to(i))], routed_v.at[q, rows(me)], out_s.at[i], out_r.at[i], to(i), q
        )

    def c_pair():
        return remote(pair_v, routed_v.at[qy, rows(me)], pair_s, pair_r, to(twin), q)

    def c_agy(i):
        block = routed_v.at[q, rows(source(i))]
        return remote(block, block, agy_s.at[i], agy_r.at[i], me, qy)

    def c_agd(i):
        block = routed_v.at[q, rows(source(i))]
        return remote(block, block, agd_s.at[i], agd_r.at[i], me, qd)

    def c_fwd(i):
        block = routed_v.at[qy, rows(source(i))]
        return remote(block, block, fwd_s.at[i], fwd_r.at[i], me, qd)

    def c_core(i, h):
        return remote(
            part_v.at[(qd, qdy)[h], rows(source(i))],
            core_v.at[h, rows(source(i))],
            core_s.at[h, i],
            core_r.at[h, i],
            me,
            qd,
        )

    def c_y(i):
        block = rows(source(i))
        return remote(ysend_v.at[block], yrecv_v.at[block], y_s.at[i], y_r.at[i], me, qy)

    def c_ret(i):
        return remote(
            back_v.at[rows(source(i))], ret_v.at[rows(me)], ret_s.at[i], ret_r.at[i], source(i), q
        )

    ids = ids_ref[...]
    experts = n
    e_iota = lax.broadcasted_iota(jnp.int32, (experts, tokens), 0)
    hits = [e_iota == ids[k : k + 1, :] for k in range(top)]
    named = hits[0].astype(F32)
    for k in range(1, top):
        named = named + hits[k].astype(F32)
    earlier = (
        lax.broadcasted_iota(jnp.int32, (tokens, tokens), 0)
        < lax.broadcasted_iota(jnp.int32, (tokens, tokens), 1)
    ).astype(F32).astype(BF16)
    before = mm(named.astype(BF16), earlier)
    place = [
        jnp.sum(jnp.where(hits[k], before, 0.0), axis=0, keepdims=True)
        + ids[k : k + 1, :].astype(F32) * cap
        for k in range(top)
    ]
    slot_iota = lax.broadcasted_iota(jnp.int32, (cap, tokens), 0)

    def select(block):
        slot = (slot_iota + block * cap).astype(F32)
        mask = jnp.zeros((cap, tokens), F32)
        weight = jnp.zeros((cap, tokens), F32)
        for k in range(top):
            same = slot == place[k]
            mask = jnp.where(same, 1.0, mask)
            weight = jnp.where(same, wts_ref[k : k + 1, :], weight)
        mask = mask.astype(BF16)
        sel_v[rows(block), :] = mask
        return mask, jnp.sum(weight, axis=1, keepdims=True)

    pl.semaphore_wait(barrier, n - 1 + 2)

    def build(i, carry):
        mask, weight = select(to(i))
        sent_v[rows(to(i)), :] = (weight * mm(mask, gathered(cot_ref, q))).astype(BF16)
        c_out(i).start()

        @pl.when(i == twin)
        def _():
            pair_v[...] = (weight * mm(mask, gathered(cot_ref, qy))).astype(BF16)
            c_pair().start()

        return carry

    lax.fori_loop(1, 3, build, 0)
    mask, weight = select(me)
    for part in range(tp):
        routed_v[part, rows(me), :] = (weight * mm(mask, gathered(cot_ref, part))).astype(BF16)

    for load in loads:
        load.wait()

    chunk = min(slots, 256)

    def ahead(some):
        pre_g[some, :] = mm(x_v[some, :], wg_v[...])
        pre_u[some, :] = mm(x_v[some, :], wu_v[...])

    def forward(i, carry):
        ahead(pl.ds(pl.multiple_of(i * chunk, chunk), chunk))
        return carry

    def stage_experts(j):
        block = rows(source(j))
        total = mm(routed_v[0, block, :], gathered(wd_v, 0), NT)
        for part in range(1, tp):
            total = total + mm(routed_v[part, block, :], gathered(wd_v, part), NT)
        gate = pre_g[block, :]
        up = pre_u[block, :]
        sig = jax.nn.sigmoid(gate)
        swish = gate * sig
        hid_v[block, :] = (swish * up).astype(BF16)
        g_gate = (total * up * sig * (1.0 + gate * (1.0 - sig))).astype(BF16)
        g_up = (total * swish).astype(BF16)
        gpg_v[block, :] = g_gate
        gpu_v[block, :] = g_up
        for u in range(2 * tp):
            some = slice(u * du, (u + 1) * du)
            part_v[u % tp, block, u // tp * du : (u // tp + 1) * du] = (
                mm(g_gate, wg_v[some, :], NT) + mm(g_up, wu_v[some, :], NT)
            ).astype(BF16)
        c_core(j, 1).start()
        c_core(j, 0).start()

    def share(j):
        c_out(j).wait_recv()
        c_agd(j).start()

        @pl.when(j != twin)
        def _():
            c_agy(j).start()

    def pass_on(j):
        @pl.when(j != twin)
        def _():
            c_agy(j).wait_recv()

        @pl.when(j == twin)
        def _():
            c_pair().wait_recv()

        c_fwd(j).start()

    def stage_cores(j):
        block = rows(source(j))
        c_core(j, 1).wait_recv()
        ysend_v[block, :] = (
            part_v[qy, block, :].astype(F32) + core_v[1, block, :].astype(F32)
        ).astype(BF16)
        c_y(j).start()

    def stage_return(j):
        block = rows(source(j))
        c_core(j, 0).wait_recv()
        c_y(j).wait_recv()
        total = (
            part_v[q, block, :].astype(F32)
            + core_v[0, block, :].astype(F32)
            + yrecv_v[block, :].astype(F32)
        ).astype(BF16)

        @pl.when(j == 0)
        def _():
            ret_v[block, :] = total

        @pl.when(j > 0)
        def _():
            back_v[block, :] = total
            c_ret(j).start()

    def experts(j):
        c_agd(j).wait_recv()
        c_fwd(j).wait_recv()
        stage_experts(j)

    def pipeline(t, carry):
        @pl.when(t < n - 1)
        def _():
            share(t + 1)

        @pl.when(t < n - 4)
        def _():
            build(t + 4, 0)

        experts(t)

        stage_return(t - 1)

        stage_cores(t)

        @pl.when(t < n - 1)
        def _():
            pass_on(t + 1)

        return carry

    ahead(rows(me))
    stage_experts(0)
    build(3, 0)
    lax.fori_loop(0, slots // chunk // 2, forward, 0)
    stage_cores(0)
    share(1)
    build(4, 0)
    lax.fori_loop(slots // chunk // 2, slots // chunk, forward, 0)
    pass_on(1)
    lax.fori_loop(1, n, pipeline, 0)

    for part in range(tp):
        both = mm(hid_v[...], routed_v[part], TN).astype(BF16)
        gd_v[:, part * du : (part + 1) * du] = both[:, :du]
        gd_v[:, (part + tp) * du : (part + tp + 1) * du] = both[:, du:]
    save_gd = pltpu.make_async_copy(gd_v, gd_hbm.at[0], save_sem.at[1])
    save_gd.start()
    piece = min(width, 512)

    def weights(i, carry):
        some = pl.ds(pl.multiple_of(i * piece, piece), piece)
        flipped = x_v[:, some]
        gg_v[some, :] = mm(flipped, gpg_v[...], TN).astype(BF16)
        gu_v[some, :] = mm(flipped, gpu_v[...], TN).astype(BF16)
        return carry

    lax.fori_loop(0, width // piece // 2, weights, 0)
    stage_return(n - 1)
    lax.fori_loop(width // piece // 2, width // piece, weights, 0)
    save_gg = pltpu.make_async_copy(gg_v, gg_hbm.at[0], save_sem.at[2])
    save_gg.start()
    save_gu = pltpu.make_async_copy(gu_v, gu_hbm.at[0], save_sem.at[3])
    save_gu.start()

    def wait_ret(i, carry):
        c_ret(i).wait_recv()
        return carry

    lax.fori_loop(1, n, wait_ret, 0)
    mine = (gathered(cot_ref, q).astype(F32) + mm(sel_v[...], ret_v[...], TN)).astype(BF16)
    mid_v[q] = mine

    def half_of(part, h):
        return mid_v.at[part, :, h * du : (h + 1) * du]

    mid_y = [remote(half_of(q, h), half_of(q, h), mid_s.at[h], mid_r.at[h], me, qy) for h in (0, 1)]
    mid_f = [
        remote(half_of(qy, h), half_of(qy, h), mid_s.at[h + 2], mid_r.at[h + 2], me, qd)
        for h in (0, 1)
    ]
    mid_d = remote(mid_v.at[q], mid_v.at[q], mid_s.at[4], mid_r.at[4], me, qd)
    mid_y[0].start()
    mid_d.start()
    mid_y[1].start()

    gate_in = gin_ref[...].astype(F32)
    conv_sum = csum_ref[...].astype(F32)
    mixed = (gate_in * conv_sum).astype(BF16)
    own_rows = width // n
    owners = n // (2 * tp)

    def owned(block):
        return pl.ds(pl.multiple_of(block * own_rows, own_rows), own_rows)

    def c_term(block, slot):
        return remote(
            term_v.at[owned(block)], terms_v.at[slot], term_s.at[block], term_r.at[slot], block, q
        )

    def send_terms(part, h):
        some = unit(part, h)
        term_v[some, :] = mm(mid_v[part, :, h * du : (h + 1) * du], mixed, TN).astype(BF16)

        def send(i, carry):
            block = (part + h * tp) * owners + i

            @pl.when(block != me)
            def _():
                c_term(block, me).start()

            return carry

        lax.fori_loop(0, owners, send, 0)

    send_terms(q, 0)
    send_terms(q, 1)
    mid_d.wait_recv()
    send_terms(qd, 0)
    send_terms(qd, 1)
    mid_y[0].wait_recv()
    mid_f[0].start()
    send_terms(qy, 0)
    mid_f[0].wait_recv()
    send_terms(qdy, 0)
    mid_y[1].wait_recv()
    mid_f[1].start()
    send_terms(qy, 1)
    mid_f[1].wait_recv()
    save_gi = [
        pltpu.make_async_copy(
            mid_v.at[
                (2 * q + i) % tp,
                :,
                pl.ds(pl.multiple_of((2 * q + i) // tp * du, du), du),
            ],
            gi_hbm.at[:, i * du : (i + 1) * du],
            save_sem.at[4 * i],
        )
        for i in range(2)
    ]
    for save in save_gi:
        save.start()
    grad_mixed = jnp.zeros((tokens, mixed.shape[1]), F32)
    for u in range(2 * tp):
        grad_mixed = grad_mixed + mm(
            mid_v[u % tp, :, u // tp * du : (u // tp + 1) * du], ow_ref[u * du : (u + 1) * du, :]
        )
    ext_v[:tokens, :] = grad_mixed * gate_in
    edge = halo_v.shape[0]
    halo = remote(ext_v.at[pl.ds(0, edge)], halo_v, halo_s, halo_r, (me - 1 + n) % n, q)
    halo.start()
    send_terms(qdy, 1)
    ggi_out[...] = (grad_mixed * conv_sum).astype(BF16)

    halo.wait_recv()
    ext_v[tokens:, :] = jnp.where(me == n - 1, 0.0, halo_v[...])
    taps = taps_ref[...]
    grad_prod = (
        taps[0:1, :] * ext_v[2 : tokens + 2, :]
        + taps[1:2, :] * ext_v[1 : tokens + 1, :]
        + taps[2:3, :] * ext_v[:tokens, :]
    )
    gcc_out[...] = (grad_prod * cv_ref[...].astype(F32)).astype(BF16)
    gcv_out[...] = (grad_prod * cc_ref[...].astype(F32)).astype(BF16)

    def add_term(i, total):
        other = (me + i) % n
        c_term(other, other).wait_recv()
        return total + terms_v[other].astype(F32)

    gow_out[...] = lax.fori_loop(1, n, add_term, term_v[owned(me), :].astype(F32))

    def drain(i, carry):
        c_out(i).wait_send()
        c_agd(i).wait_send()

        @pl.when(i != twin)
        def _():
            c_agy(i).wait_send()

        c_fwd(i).wait_send()
        c_ret(i).wait_send()
        c_term((me + i) % n, me).wait_send()
        return carry

    lax.fori_loop(1, n, drain, 0)
    c_pair().wait_send()

    def drain_all(i, carry):
        c_core(i, 0).wait_send()
        c_core(i, 1).wait_send()
        c_y(i).wait_send()
        return carry

    lax.fori_loop(0, n, drain_all, 0)
    mid_d.wait_send()
    for h in (0, 1):
        mid_y[h].wait_send()
        mid_f[h].wait_send()
    halo.wait_send()
    for save in (*save_gi, save_gd, save_gg, save_gu):
        save.wait()


def move(*refs):
    count = (len(refs) - 2) // 3
    sources, targets, held = refs[:count], refs[count : 2 * count], refs[2 * count : 3 * count]
    in_sem, out_sem = refs[-2:]
    ins = [pltpu.make_async_copy(sources[i], held[i], in_sem.at[i]) for i in range(count)]
    outs = [pltpu.make_async_copy(held[i], targets[i], out_sem.at[i]) for i in range(count)]
    for copy in ins:
        copy.start()
    for i in range(count):
        ins[i].wait()
        outs[i].start()
    for copy in outs:
        copy.wait()


def moved(arrays):
    count = len(arrays)
    hbm = pl.BlockSpec(memory_space=pl.ANY)
    return pl.pallas_call(
        move,
        out_shape=tuple(jax.ShapeDtypeStruct(a.shape, a.dtype) for a in arrays),
        in_specs=[hbm] * count,
        out_specs=(hbm,) * count,
        scratch_shapes=[pltpu.VMEM(a.shape, a.dtype) for a in arrays]
        + [pltpu.SemaphoreType.DMA((count,))] * 2,
        compiler_params=pltpu.CompilerParams(vmem_limit_bytes=60 * 1024 * 1024),
    )(*arrays)


def body(
    cotangent,
    route_ids,
    route_weights,
    expert_inputs,
    gate_weight,
    up_weight,
    down_weight,
    out_weight,
    gate_in,
    conv_sum,
    conv_c,
    conv_v,
    conv_taps,
):
    n = lax.axis_size("sp")
    tp = lax.axis_size("tp")
    tokens, width = cotangent.shape
    slots = expert_inputs.shape[1]
    hidden = gate_weight.shape[2]
    chans = gate_in.shape[1]
    dq = width // tp
    vmem = pl.BlockSpec(memory_space=pltpu.VMEM)
    hbm = pl.BlockSpec(memory_space=pl.ANY)
    dma = pltpu.SemaphoreType.DMA
    results = pl.pallas_call(
        functools.partial(kernel, n, tp),
        out_shape=(
            jax.ShapeDtypeStruct((tokens, dq), BF16),
            jax.ShapeDtypeStruct(gate_weight.shape, BF16),
            jax.ShapeDtypeStruct(up_weight.shape, BF16),
            jax.ShapeDtypeStruct(down_weight.shape, BF16),
            jax.ShapeDtypeStruct((width // n, chans), F32),
            jax.ShapeDtypeStruct((tokens, chans), BF16),
            jax.ShapeDtypeStruct((tokens, chans), BF16),
            jax.ShapeDtypeStruct((tokens, chans), BF16),
        ),
        in_specs=[vmem] * 3 + [hbm] * 4 + [vmem] * 6,
        out_specs=(hbm,) * 4 + (vmem,) * 4,
        scratch_shapes=[
            pltpu.VMEM((slots, width), BF16),
            pltpu.VMEM((width, hidden), BF16),
            pltpu.VMEM((width, hidden), BF16),
            pltpu.VMEM((hidden, width), BF16),
            pltpu.VMEM((slots, tokens), BF16),
            pltpu.VMEM((slots, dq), BF16),
            pltpu.VMEM((slots // n, dq), BF16),
            pltpu.VMEM((tp, slots, dq), BF16),
            pltpu.VMEM((slots, hidden), F32),
            pltpu.VMEM((slots, hidden), F32),
            pltpu.VMEM((slots, hidden), BF16),
            pltpu.VMEM((slots, hidden), BF16),
            pltpu.VMEM((slots, hidden), BF16),
            pltpu.VMEM((tp, slots, dq), BF16),
            pltpu.VMEM((2, slots, dq), BF16),
            pltpu.VMEM((slots, dq), BF16),
            pltpu.VMEM((slots, dq), BF16),
            pltpu.VMEM((slots, dq), BF16),
            pltpu.VMEM((slots, dq), BF16),
            pltpu.VMEM((tp, tokens, dq), BF16),
            pltpu.VMEM((width, chans), BF16),
            pltpu.VMEM((n, width // n, chans), BF16),
            pltpu.VMEM((tokens + 8, chans), F32),
            pltpu.VMEM((8, chans), F32),
            pltpu.VMEM((width, hidden), BF16),
            pltpu.VMEM((width, hidden), BF16),
            pltpu.VMEM((hidden, width), BF16),
            dma((4,)),
            dma((5,)),
            dma((n,)),
            dma((n,)),
            dma(()),
            dma(()),
            dma((n,)),
            dma((n,)),
            dma((n,)),
            dma((n,)),
            dma((n,)),
            dma((n,)),
            dma((2, n)),
            dma((2, n)),
            dma((n,)),
            dma((n,)),
            dma((n,)),
            dma((n,)),
            dma((5,)),
            dma((5,)),
            dma((n,)),
            dma((n,)),
            dma(()),
            dma(()),
        ],
        compiler_params=pltpu.CompilerParams(
            collective_id=0, has_side_effects=True, vmem_limit_bytes=60 * 1024 * 1024
        ),
    )(
        route_ids.T,
        route_weights.T,
        cotangent,
        expert_inputs,
        gate_weight,
        up_weight,
        down_weight,
        out_weight,
        gate_in,
        conv_sum,
        conv_c,
        conv_v,
        conv_taps,
    )
    return moved(results)


def solution(mesh):
    placed = (
        P("sp", None),
        P("sp", None),
        P("sp", None),
        P("sp", None, None),
        P("sp", None, "tp"),
        P("sp", None, "tp"),
        P("sp", "tp", None),
        P(None, "tp"),
        P("sp", "tp"),
        P("sp", "tp"),
        P("sp", "tp"),
        P("sp", "tp"),
        P(None, "tp"),
    )
    return jax.shard_map(
        body,
        mesh=mesh,
        in_specs=placed,
        out_specs=(
            P("sp", "tp"),
            P("sp", None, "tp"),
            P("sp", None, "tp"),
            P("sp", "tp", None),
            P("sp", "tp"),
            P("sp", "tp"),
            P("sp", "tp"),
            P("sp", "tp"),
        ),
        check_vma=False,
    )
```

```python
import functools

import jax
import jax.numpy as jnp
from jax import lax
from jax.experimental import pallas as pl
from jax.experimental.pallas import tpu as pltpu
from jax.sharding import PartitionSpec as P

F32 = jnp.float32
BF16 = jnp.bfloat16
NT = (((1,), (1,)), ((), ()))
TN = (((0,), (0,)), ((), ()))


def mm(a, b, dims=(((1,), (0,)), ((), ()))):
    return lax.dot_general(a, b, dims, preferred_element_type=F32)


def kernel(
    n,
    tp,
    ids_hbm,
    wts_hbm,
    cot_hbm,
    x_hbm,
    wg_hbm,
    wu_hbm,
    wd_hbm,
    ow_hbm,
    gin_hbm,
    csum_hbm,
    cc_hbm,
    cv_hbm,
    taps_hbm,
    gi_out,
    gg_out,
    gu_out,
    gd_out,
    gow_out,
    ggi_out,
    gcc_out,
    gcv_out,
    ids_ref,
    wts_ref,
    cot_ref,
    ow_ref,
    gin_ref,
    csum_ref,
    cc_ref,
    cv_ref,
    taps_ref,
    x_v,
    wg_v,
    wu_v,
    wd_v,
    sel_v,
    sent_v,
    pair_v,
    routed_v,
    pre_g,
    pre_u,
    hid_v,
    gpg_v,
    gpu_v,
    part_v,
    core_v,
    ysend_v,
    yrecv_v,
    back_v,
    ret_v,
    mid_v,
    term_v,
    terms_v,
    ext_v,
    halo_v,
    load_sem,
    side_sem,
    out_s,
    out_r,
    pair_s,
    pair_r,
    agy_s,
    agy_r,
    agd_s,
    agd_r,
    fwd_s,
    fwd_r,
    core_s,
    core_r,
    y_s,
    y_r,
    ret_s,
    ret_r,
    mid_s,
    mid_r,
    term_s,
    term_r,
    halo_s,
    halo_r,
):
    me = lax.axis_index("sp")
    q = lax.axis_index("tp")
    qd = q + 1 - 2 * (q % 2)
    qy = (q + tp // 2) % tp
    qdy = (qd + tp // 2) % tp
    tokens, width = cot_ref.shape
    slots = x_v.shape[0]
    cap = slots // n
    dq = width // tp
    du = dq // 2
    top = ids_ref.shape[0]

    barrier = pltpu.get_barrier_semaphore()

    def greet(i, carry):
        pl.semaphore_signal(
            barrier, inc=1, device_id=((me + i) % n, q), device_id_type=pl.DeviceIdType.MESH
        )
        return carry

    lax.fori_loop(1, n, greet, 0)
    for other in (qd, qy):
        pl.semaphore_signal(
            barrier, inc=1, device_id=(me, other), device_id_type=pl.DeviceIdType.MESH
        )

    first_loads = [
        pltpu.make_async_copy(src, dst, side_sem.at[i])
        for i, (src, dst) in enumerate(
            ((ids_hbm, ids_ref), (wts_hbm, wts_ref), (cot_hbm, cot_ref))
        )
    ]
    loads = [
        pltpu.make_async_copy(src.at[0], dst, load_sem.at[i])
        for i, (src, dst) in enumerate(
            ((wg_hbm, wg_v), (wu_hbm, wu_v), (wd_hbm, wd_v), (x_hbm, x_v))
        )
    ]
    late_loads = [
        pltpu.make_async_copy(src, dst, side_sem.at[i + 3])
        for i, (src, dst) in enumerate(
            (
                (ow_hbm, ow_ref),
                (gin_hbm, gin_ref),
                (csum_hbm, csum_ref),
                (cc_hbm, cc_ref),
                (cv_hbm, cv_ref),
                (taps_hbm, taps_ref),
            )
        )
    ]

    for load in (*first_loads, *loads, *late_loads):
        load.start()

    def rows(block):
        return pl.ds(pl.multiple_of(block * cap, cap), cap)

    def unit(part, side):
        return pl.ds(pl.multiple_of((part + side * tp) * du, du), du)

    def gathered(ref, part):
        return jnp.concatenate([ref[:, unit(part, 0)], ref[:, unit(part, 1)]], axis=1)

    def remote(src, dst, ssem, rsem, sp_id, tp_id):
        return pltpu.make_async_remote_copy(
            src_ref=src,
            dst_ref=dst,
            send_sem=ssem,
            recv_sem=rsem,
            device_id=(sp_id, tp_id),
            device_id_type=pl.DeviceIdType.MESH,
        )

    half = n // 2
    pairs = half // 2
    side, low = me // half, me % half
    pair, member = low // 2, low % 2

    def index(p):
        far = jnp.where(p == 2, half, half + p - 3)
        near = jnp.where(p < 2, p, jnp.where(p == 3, 2, p - half))
        return jnp.where((p == 2) | ((p > 3) & (p < half + 3)), far, near)

    def across_at(p):
        return index(p) >= half

    def step(p):
        i = index(p)
        across = jnp.where(i >= half, 1, 0)
        turn = i % half
        return (side + across) % 2 * half, turn // 2, turn % 2

    def to(i):
        base, hop, swap = step(i)
        return base + (pair + hop) % pairs * 2 + (member + swap) % 2

    def source(i):
        base, hop, swap = step(i)
        return base + (pair - hop + pairs) % pairs * 2 + (member + swap) % 2

    def c_out(i):
        return remote(
            sent_v.at[rows(to(i))], routed_v.at[q, rows(me)], out_s.at[i], out_r.at[i], to(i), q
        )

    def c_pair(i):
        return remote(
            pair_v.at[rows(to(i))],
            routed_v.at[qy, rows(me)],
            pair_s.at[i],
            pair_r.at[i],
            to(i),
            q,
        )

    def c_agy(i):
        block = routed_v.at[q, rows(source(i))]
        return remote(block, block, agy_s.at[i], agy_r.at[i], me, qy)

    def c_agd(i):
        block = routed_v.at[q, rows(source(i))]
        return remote(block, block, agd_s.at[i], agd_r.at[i], me, qd)

    def c_fwd(i):
        block = routed_v.at[qy, rows(source(i))]
        return remote(block, block, fwd_s.at[i], fwd_r.at[i], me, qd)

    def c_core(i, h):
        return remote(
            part_v.at[(qd, qdy)[h], rows(source(i))],
            core_v.at[h, rows(source(i))],
            core_s.at[h, i],
            core_r.at[h, i],
            me,
            qd,
        )

    def c_y(i):
        block = rows(source(i))
        return remote(ysend_v.at[block], yrecv_v.at[block], y_s.at[i], y_r.at[i], me, qy)

    def c_ret(i):
        return remote(
            back_v.at[rows(source(i))], ret_v.at[rows(me)], ret_s.at[i], ret_r.at[i], source(i), q
        )

    for load in first_loads:
        load.wait()
    ids = ids_ref[...]
    experts = n
    e_iota = lax.broadcasted_iota(jnp.int32, (experts, tokens), 0)
    hits = [e_iota == ids[k : k + 1, :] for k in range(top)]
    named = hits[0].astype(F32)
    for k in range(1, top):
        named = named + hits[k].astype(F32)
    earlier = (
        lax.broadcasted_iota(jnp.int32, (tokens, tokens), 0)
        < lax.broadcasted_iota(jnp.int32, (tokens, tokens), 1)
    ).astype(F32).astype(BF16)
    before = mm(named.astype(BF16), earlier)
    place = [
        jnp.sum(jnp.where(hits[k], before, 0.0), axis=0, keepdims=True)
        + ids[k : k + 1, :].astype(F32) * cap
        for k in range(top)
    ]
    slot_iota = lax.broadcasted_iota(jnp.int32, (cap, tokens), 0)

    def select(block):
        slot = (slot_iota + block * cap).astype(F32)
        mask = jnp.zeros((cap, tokens), F32)
        weight = jnp.zeros((cap, tokens), F32)
        for k in range(top):
            same = slot == place[k]
            mask = jnp.where(same, 1.0, mask)
            weight = jnp.where(same, wts_ref[k : k + 1, :], weight)
        mask = mask.astype(BF16)
        sel_v[rows(block), :] = mask
        return mask, jnp.sum(weight, axis=1, keepdims=True)

    pl.semaphore_wait(barrier, n - 1 + 2)

    def build(i, carry):
        mask, weight = select(to(i))
        sent_v[rows(to(i)), :] = (weight * mm(mask, gathered(cot_ref, q))).astype(BF16)
        c_out(i).start()

        @pl.when(jnp.logical_not(across_at(i)))
        def _():
            pair_v[rows(to(i)), :] = (weight * mm(mask, gathered(cot_ref, qy))).astype(BF16)
            c_pair(i).start()

        return carry

    lax.fori_loop(1, 4, build, 0)
    mask, weight = select(me)
    for part in range(tp):
        routed_v[part, rows(me), :] = (weight * mm(mask, gathered(cot_ref, part))).astype(BF16)

    for load in loads:
        load.wait()

    chunk = min(slots, 256)

    def ahead(some):
        pre_g[some, :] = mm(x_v[some, :], wg_v[...])
        pre_u[some, :] = mm(x_v[some, :], wu_v[...])

    def forward(i, carry):
        ahead(pl.ds(pl.multiple_of(i * chunk, chunk), chunk))
        return carry

    def stage_experts(j):
        block = rows(source(j))
        total = mm(routed_v[0, block, :], gathered(wd_v, 0), NT)
        for part in range(1, tp):
            total = total + mm(routed_v[part, block, :], gathered(wd_v, part), NT)
        gate = pre_g[block, :]
        up = pre_u[block, :]
        sig = jax.nn.sigmoid(gate)
        swish = gate * sig
        hid_v[block, :] = (swish * up).astype(BF16)
        g_gate = (total * up * sig * (1.0 + gate * (1.0 - sig))).astype(BF16)
        g_up = (total * swish).astype(BF16)
        gpg_v[block, :] = g_gate
        gpu_v[block, :] = g_up
        for u in range(2 * tp):
            some = slice(u * du, (u + 1) * du)
            part_v[u % tp, block, u // tp * du : (u // tp + 1) * du] = (
                mm(g_gate, wg_v[some, :], NT) + mm(g_up, wu_v[some, :], NT)
            ).astype(BF16)
        c_core(j, 1).start()
        c_core(j, 0).start()

    def share(j):
        c_out(j).wait_recv()
        c_agd(j).start()

        @pl.when(across_at(j))
        def _():
            c_agy(j).start()

    def pass_on(j):
        @pl.when(across_at(j))
        def _():
            c_agy(j).wait_recv()

        @pl.when(jnp.logical_not(across_at(j)))
        def _():
            c_pair(j).wait_recv()

        c_fwd(j).start()

    def stage_cores(j):
        block = rows(source(j))
        c_core(j, 1).wait_recv()
        ysend_v[block, :] = (
            part_v[qy, block, :].astype(F32) + core_v[1, block, :].astype(F32)
        ).astype(BF16)
        c_y(j).start()

    def stage_return(j):
        block = rows(source(j))
        c_core(j, 0).wait_recv()
        c_y(j).wait_recv()
        total = (
            part_v[q, block, :].astype(F32)
            + core_v[0, block, :].astype(F32)
            + yrecv_v[block, :].astype(F32)
        ).astype(BF16)

        @pl.when(j == 0)
        def _():
            ret_v[block, :] = total

        @pl.when(j > 0)
        def _():
            back_v[block, :] = total
            c_ret(j).start()

    def experts(j):
        c_agd(j).wait_recv()
        c_fwd(j).wait_recv()
        stage_experts(j)

    def pipeline(t, carry):
        @pl.when(t < 4)
        def _():
            share(t + 1)

        @pl.when(t < n - 4)
        def _():
            build(t + 4, 0)

        experts(t)

        stage_cores(t)

        stage_return(t - 1)

        @pl.when(jnp.logical_and(t + 1 >= 4, t < n - 2))
        def _():
            share(t + 2)

        @pl.when(t < n - 1)
        def _():
            pass_on(t + 1)

        return carry

    ahead(rows(me))
    stage_experts(0)
    build(4, 0)
    lax.fori_loop(0, slots // chunk // 2, forward, 0)
    stage_cores(0)
    share(1)
    lax.fori_loop(slots // chunk // 2, slots // chunk, forward, 0)
    pass_on(1)
    lax.fori_loop(1, n, pipeline, 0)

    for part in range(tp):
        both = mm(hid_v[...], routed_v[part], TN).astype(BF16)
        gd_out[0, :, part * du : (part + 1) * du] = both[:, :du]
        gd_out[0, :, (part + tp) * du : (part + tp + 1) * du] = both[:, du:]
    piece = min(width, 512)

    def weights(i, carry):
        some = pl.ds(pl.multiple_of(i * piece, piece), piece)
        flipped = x_v[:, some]
        gg_out[0, some, :] = mm(flipped, gpg_v[...], TN).astype(BF16)
        gu_out[0, some, :] = mm(flipped, gpu_v[...], TN).astype(BF16)
        return carry

    lax.fori_loop(0, width // piece // 2, weights, 0)
    stage_return(n - 1)
    lax.fori_loop(width // piece // 2, width // piece, weights, 0)

    def wait_ret(i, carry):
        c_ret(i).wait_recv()
        return carry

    lax.fori_loop(1, n, wait_ret, 0)
    mine = (gathered(cot_ref, q).astype(F32) + mm(sel_v[...], ret_v[...], TN)).astype(BF16)
    mid_v[q] = mine

    def half_of(part, h):
        return mid_v.at[part, :, h * du : (h + 1) * du]

    mid_y = [remote(half_of(q, h), half_of(q, h), mid_s.at[h], mid_r.at[h], me, qy) for h in (0, 1)]
    mid_f = [
        remote(half_of(qy, h), half_of(qy, h), mid_s.at[h + 2], mid_r.at[h + 2], me, qd)
        for h in (0, 1)
    ]
    mid_d = remote(mid_v.at[q], mid_v.at[q], mid_s.at[4], mid_r.at[4], me, qd)
    mid_y[0].start()
    mid_d.start()
    mid_y[1].start()

    for load in late_loads:
        load.wait()
    gate_in = gin_ref[...].astype(F32)
    conv_sum = csum_ref[...].astype(F32)
    mixed = (gate_in * conv_sum).astype(BF16)
    own_rows = width // n
    owners = n // (2 * tp)

    def owned(block):
        return pl.ds(pl.multiple_of(block * own_rows, own_rows), own_rows)

    def c_term(block, slot):
        return remote(
            term_v.at[owned(block)], terms_v.at[slot], term_s.at[block], term_r.at[slot], block, q
        )

    def send_terms(part, h):
        some = unit(part, h)
        term_v[some, :] = mm(mid_v[part, :, h * du : (h + 1) * du], mixed, TN).astype(BF16)

        def send(i, carry):
            block = (part + h * tp) * owners + i

            @pl.when(block != me)
            def _():
                c_term(block, me).start()

            return carry

        lax.fori_loop(0, owners, send, 0)

    send_terms(q, 0)
    send_terms(q, 1)
    mid_d.wait_recv()
    send_terms(qd, 0)
    send_terms(qd, 1)
    mid_y[0].wait_recv()
    mid_f[0].start()
    send_terms(qy, 0)
    mid_f[0].wait_recv()
    send_terms(qdy, 0)
    mid_y[1].wait_recv()
    mid_f[1].start()
    send_terms(qy, 1)
    mid_f[1].wait_recv()
    grad_mixed = jnp.zeros((tokens, mixed.shape[1]), F32)
    for u in range(2 * tp):
        grad_mixed = grad_mixed + mm(
            mid_v[u % tp, :, u // tp * du : (u // tp + 1) * du], ow_ref[u * du : (u + 1) * du, :]
        )
    ext_v[:tokens, :] = grad_mixed * gate_in
    edge = halo_v.shape[0]
    halo = remote(ext_v.at[pl.ds(0, edge)], halo_v, halo_s, halo_r, (me - 1 + n) % n, q)
    halo.start()
    send_terms(qdy, 1)
    for i in range(2):
        own = 2 * q + i
        gi_out[:, i * du : (i + 1) * du] = mid_v[
            own % tp, :, pl.ds(pl.multiple_of(own // tp * du, du), du)
        ]
    ggi_out[...] = (grad_mixed * conv_sum).astype(BF16)

    halo.wait_recv()
    ext_v[tokens:, :] = jnp.where(me == n - 1, 0.0, halo_v[...])
    taps = taps_ref[...]
    grad_prod = (
        taps[0:1, :] * ext_v[2 : tokens + 2, :]
        + taps[1:2, :] * ext_v[1 : tokens + 1, :]
        + taps[2:3, :] * ext_v[:tokens, :]
    )
    gcc_out[...] = (grad_prod * cv_ref[...].astype(F32)).astype(BF16)
    gcv_out[...] = (grad_prod * cc_ref[...].astype(F32)).astype(BF16)

    def add_term(i, total):
        other = (me + i) % n
        c_term(other, other).wait_recv()
        return total + terms_v[other].astype(F32)

    gow_out[...] = lax.fori_loop(1, n, add_term, term_v[owned(me), :].astype(F32))

    def drain(i, carry):
        c_out(i).wait_send()
        c_agd(i).wait_send()

        @pl.when(across_at(i))
        def _():
            c_agy(i).wait_send()

        @pl.when(jnp.logical_not(across_at(i)))
        def _():
            c_pair(i).wait_send()

        c_fwd(i).wait_send()
        c_ret(i).wait_send()
        c_term((me + i) % n, me).wait_send()
        return carry

    lax.fori_loop(1, n, drain, 0)

    def drain_all(i, carry):
        c_core(i, 0).wait_send()
        c_core(i, 1).wait_send()
        c_y(i).wait_send()
        return carry

    lax.fori_loop(0, n, drain_all, 0)
    mid_d.wait_send()
    for h in (0, 1):
        mid_y[h].wait_send()
        mid_f[h].wait_send()
    halo.wait_send()


def move(*refs):
    count = (len(refs) - 1) // 2
    outs = [
        pltpu.make_async_copy(refs[i], refs[count + i], refs[-1].at[i]) for i in range(count)
    ]
    for copy in outs:
        copy.start()
    for copy in outs:
        copy.wait()


def moved(arrays):
    count = len(arrays)
    return pl.pallas_call(
        move,
        out_shape=tuple(jax.ShapeDtypeStruct(a.shape, a.dtype) for a in arrays),
        in_specs=[pl.BlockSpec(memory_space=pltpu.VMEM)] * count,
        out_specs=(pl.BlockSpec(memory_space=pl.ANY),) * count,
        scratch_shapes=[pltpu.SemaphoreType.DMA((count,))],
        compiler_params=pltpu.CompilerParams(vmem_limit_bytes=16000 * 1024),
    )(*arrays)


def body(
    cotangent,
    route_ids,
    route_weights,
    expert_inputs,
    gate_weight,
    up_weight,
    down_weight,
    out_weight,
    gate_in,
    conv_sum,
    conv_c,
    conv_v,
    conv_taps,
):
    n = lax.axis_size("sp")
    tp = lax.axis_size("tp")
    tokens, width = cotangent.shape
    slots = expert_inputs.shape[1]
    hidden = gate_weight.shape[2]
    chans = gate_in.shape[1]
    top = route_ids.shape[1]
    dq = width // tp
    vmem = pl.BlockSpec(memory_space=pltpu.VMEM)
    hbm = pl.BlockSpec(memory_space=pl.ANY)
    dma = pltpu.SemaphoreType.DMA
    results = pl.pallas_call(
        functools.partial(kernel, n, tp),
        out_shape=(
            pltpu.VMEM((tokens, dq), BF16),
            pltpu.VMEM(gate_weight.shape, BF16),
            pltpu.VMEM(up_weight.shape, BF16),
            pltpu.VMEM(down_weight.shape, BF16),
            pltpu.VMEM((width // n, chans), F32),
            pltpu.VMEM((tokens, chans), BF16),
            pltpu.VMEM((tokens, chans), BF16),
            pltpu.VMEM((tokens, chans), BF16),
        ),
        in_specs=[hbm] * 13,
        out_specs=(vmem,) * 8,
        scratch_shapes=[
            pltpu.VMEM((top, tokens), jnp.int32),
            pltpu.VMEM((top, tokens), F32),
            pltpu.VMEM((tokens, width), BF16),
            pltpu.VMEM((width, chans), BF16),
            pltpu.VMEM((tokens, chans), BF16),
            pltpu.VMEM((tokens, chans), BF16),
            pltpu.VMEM((tokens, chans), BF16),
            pltpu.VMEM((tokens, chans), BF16),
            pltpu.VMEM(conv_taps.shape, F32),
            pltpu.VMEM((slots, width), BF16),
            pltpu.VMEM((width, hidden), BF16),
            pltpu.VMEM((width, hidden), BF16),
            pltpu.VMEM((hidden, width), BF16),
            pltpu.VMEM((slots, tokens), BF16),
            pltpu.VMEM((slots, dq), BF16),
            pltpu.VMEM((slots, dq), BF16),
            pltpu.VMEM((tp, slots, dq), BF16),
            pltpu.VMEM((slots, hidden), F32),
            pltpu.VMEM((slots, hidden), F32),
            pltpu.VMEM((slots, hidden), BF16),
            pltpu.VMEM((slots, hidden), BF16),
            pltpu.VMEM((slots, hidden), BF16),
            pltpu.VMEM((tp, slots, dq), BF16),
            pltpu.VMEM((2, slots, dq), BF16),
            pltpu.VMEM((slots, dq), BF16),
            pltpu.VMEM((slots, dq), BF16),
            pltpu.VMEM((slots, dq), BF16),
            pltpu.VMEM((slots, dq), BF16),
            pltpu.VMEM((tp, tokens, dq), BF16),
            pltpu.VMEM((width, chans), BF16),
            pltpu.VMEM((n, width // n, chans), BF16),
            pltpu.VMEM((tokens + 8, chans), F32),
            pltpu.VMEM((8, chans), F32),
            dma((4,)),
            dma((9,)),
            dma((n,)),
            dma((n,)),
            dma((n,)),
            dma((n,)),
            dma((n,)),
            dma((n,)),
            dma((n,)),
            dma((n,)),
            dma((n,)),
            dma((n,)),
            dma((2, n)),
            dma((2, n)),
            dma((n,)),
            dma((n,)),
            dma((n,)),
            dma((n,)),
            dma((5,)),
            dma((5,)),
            dma((n,)),
            dma((n,)),
            dma(()),
            dma(()),
        ],
        compiler_params=pltpu.CompilerParams(
            collective_id=0, has_side_effects=True, vmem_limit_bytes=61696 * 1024
        ),
    )(
        route_ids.T,
        route_weights.T,
        cotangent,
        expert_inputs,
        gate_weight,
        up_weight,
        down_weight,
        out_weight,
        gate_in,
        conv_sum,
        conv_c,
        conv_v,
        conv_taps,
    )
    return moved(results)


def solution(mesh):
    placed = (
        P("sp", None),
        P("sp", None),
        P("sp", None),
        P("sp", None, None),
        P("sp", None, "tp"),
        P("sp", None, "tp"),
        P("sp", "tp", None),
        P(None, "tp"),
        P("sp", "tp"),
        P("sp", "tp"),
        P("sp", "tp"),
        P("sp", "tp"),
        P(None, "tp"),
    )
    return jax.shard_map(
        body,
        mesh=mesh,
        in_specs=placed,
        out_specs=(
            P("sp", "tp"),
            P("sp", None, "tp"),
            P("sp", None, "tp"),
            P("sp", "tp", None),
            P("sp", "tp"),
            P("sp", "tp"),
            P("sp", "tp"),
            P("sp", "tp"),
        ),
        check_vma=False,
    )
```

```python
import functools

import jax
import jax.numpy as jnp
from jax import lax
from jax.experimental import pallas as pl
from jax.experimental.pallas import tpu as pltpu
from jax.sharding import PartitionSpec as P

F32 = jnp.float32
BF16 = jnp.bfloat16
NT = (((1,), (1,)), ((), ()))
TN = (((0,), (0,)), ((), ()))


def mm(a, b, dims=(((1,), (0,)), ((), ()))):
    return lax.dot_general(a, b, dims, preferred_element_type=F32)


def kernel(
    n,
    tp,
    ids_hbm,
    wts_hbm,
    cot_hbm,
    x_hbm,
    wg_hbm,
    wu_hbm,
    wd_hbm,
    ow_hbm,
    gin_hbm,
    csum_hbm,
    cc_hbm,
    cv_hbm,
    taps_hbm,
    gi_out,
    gg_out,
    gu_out,
    gd_out,
    gow_out,
    ggi_out,
    gcc_out,
    gcv_out,
    ids_ref,
    wts_ref,
    cot_ref,
    ow_ref,
    gin_ref,
    csum_ref,
    cc_ref,
    cv_ref,
    taps_ref,
    x_v,
    wg_v,
    wu_v,
    wd_v,
    sel_v,
    sent_v,
    pair_v,
    routed_v,
    pre_g,
    pre_u,
    hid_v,
    gpg_v,
    gpu_v,
    part_v,
    core_v,
    ysend_v,
    yrecv_v,
    back_v,
    ret_v,
    mid_v,
    term_v,
    terms_v,
    ext_v,
    halo_v,
    load_sem,
    side_sem,
    out_s,
    pair_s,
    agy_s,
    agd_s,
    fwd_s,
    core_s,
    y_s,
    ret_s,
    term_s,
    mid_s,
    halo_s,
    out_r,
    agy_r,
    core_in,
    core_r,
    y_r,
    ret_r,
    term_r,
    mid_r,
    halo_r,
):
    me = lax.axis_index("sp")
    q = lax.axis_index("tp")
    qd = q + 1 - 2 * (q % 2)
    qy = (q + tp // 2) % tp
    qdy = (qd + tp // 2) % tp
    tokens, width = cot_ref.shape
    slots = x_v.shape[0]
    cap = slots // n
    dq = width // tp
    du = dq // 2
    top = ids_ref.shape[0]

    barrier = pltpu.get_barrier_semaphore()

    def greet(i, carry):
        pl.semaphore_signal(
            barrier, inc=1, device_id=((me + i) % n, q), device_id_type=pl.DeviceIdType.MESH
        )
        return carry

    lax.fori_loop(1, n, greet, 0)
    for other in (qd, qy):
        pl.semaphore_signal(
            barrier, inc=1, device_id=(me, other), device_id_type=pl.DeviceIdType.MESH
        )

    first_loads = [
        pltpu.make_async_copy(src, dst, side_sem.at[i])
        for i, (src, dst) in enumerate(
            ((ids_hbm, ids_ref), (wts_hbm, wts_ref), (cot_hbm, cot_ref))
        )
    ]
    loads = [
        pltpu.make_async_copy(src.at[0], dst, load_sem.at[i])
        for i, (src, dst) in enumerate(
            ((wg_hbm, wg_v), (wu_hbm, wu_v), (wd_hbm, wd_v), (x_hbm, x_v))
        )
    ]
    late_loads = [
        pltpu.make_async_copy(src, dst, side_sem.at[i + 3])
        for i, (src, dst) in enumerate(
            (
                (ow_hbm, ow_ref),
                (gin_hbm, gin_ref),
                (csum_hbm, csum_ref),
                (cc_hbm, cc_ref),
                (cv_hbm, cv_ref),
                (taps_hbm, taps_ref),
            )
        )
    ]

    for load in (*first_loads, *loads, *late_loads):
        load.start()

    def rows(block):
        return pl.ds(pl.multiple_of(block * cap, cap), cap)

    def unit(part, side):
        return pl.ds(pl.multiple_of((part + side * tp) * du, du), du)

    def gathered(ref, part):
        return jnp.concatenate([ref[:, unit(part, 0)], ref[:, unit(part, 1)]], axis=1)

    def remote(src, dst, ssem, rsem, sp_id, tp_id):
        return pltpu.make_async_remote_copy(
            src_ref=src,
            dst_ref=dst,
            send_sem=ssem,
            recv_sem=rsem,
            device_id=(sp_id, tp_id),
            device_id_type=pl.DeviceIdType.MESH,
        )

    half = n // 2
    pairs = half // 2
    side, low = me // half, me % half
    pair, member = low // 2, low % 2

    def index(p):
        swapped = jnp.where((p == half + 1) | (p == half + 2), 2 * half - p, p - 3)
        far = half + jnp.where(p == 2, 0, swapped)
        near = jnp.where(p < 2, p, jnp.where(p == 3, 2, p - half))
        return jnp.where((p == 2) | ((p > 3) & (p < half + 3)), far, near)

    def across_at(p):
        return index(p) >= half

    def step(p):
        i = index(p)
        across = jnp.where(i >= half, 1, 0)
        turn = i % half
        return (side + across) % 2 * half, turn // 2, turn % 2

    def to(i):
        base, hop, swap = step(i)
        return base + (pair + hop) % pairs * 2 + (member + swap) % 2

    def source(i):
        base, hop, swap = step(i)
        return base + (pair - hop + pairs) % pairs * 2 + (member + swap) % 2

    def c_out(i):
        return remote(
            sent_v.at[rows(to(i))], routed_v.at[q, rows(me)], out_s, out_r.at[i], to(i), q
        )

    def c_pair(i):
        return remote(
            pair_v.at[rows(to(i))],
            routed_v.at[qy, rows(me)],
            pair_s,
            agy_r.at[i],
            to(i),
            q,
        )

    def c_agy(i):
        block = routed_v.at[q, rows(source(i))]
        return remote(block, block, agy_s, agy_r.at[i], me, qy)

    def c_agd(i):
        block = routed_v.at[q, rows(source(i))]
        return remote(block, block, agd_s, core_in.at[i], me, qd)

    def c_fwd(i):
        block = routed_v.at[qy, rows(source(i))]
        return remote(block, block, fwd_s, core_in.at[i], me, qd)

    def c_core(i, h):
        return remote(
            part_v.at[(qd, qdy)[h], rows(source(i))],
            core_v.at[h, rows(source(i))],
            core_s,
            core_r.at[h, i],
            me,
            qd,
        )

    def c_y(i):
        block = rows(source(i))
        return remote(ysend_v.at[block], yrecv_v.at[block], y_s, y_r.at[i], me, qy)

    def c_ret(i):
        return remote(
            back_v.at[rows(source(i))], ret_v.at[rows(me)], ret_s, ret_r, source(i), q
        )

    for load in first_loads:
        load.wait()
    ids = ids_ref[...]
    experts = n
    e_iota = lax.broadcasted_iota(jnp.int32, (experts, tokens), 0)
    hits = [e_iota == ids[k : k + 1, :] for k in range(top)]
    named = hits[0].astype(F32)
    for k in range(1, top):
        named = named + hits[k].astype(F32)
    earlier = (
        lax.broadcasted_iota(jnp.int32, (tokens, tokens), 0)
        < lax.broadcasted_iota(jnp.int32, (tokens, tokens), 1)
    ).astype(F32).astype(BF16)
    before = mm(named.astype(BF16), earlier)
    place = [
        jnp.sum(jnp.where(hits[k], before, 0.0), axis=0, keepdims=True)
        + ids[k : k + 1, :].astype(F32) * cap
        for k in range(top)
    ]
    slot_iota = lax.broadcasted_iota(jnp.int32, (cap, tokens), 0)

    def select(block):
        slot = (slot_iota + block * cap).astype(F32)
        mask = jnp.zeros((cap, tokens), F32)
        weight = jnp.zeros((cap, tokens), F32)
        for k in range(top):
            same = slot == place[k]
            mask = jnp.where(same, 1.0, mask)
            weight = jnp.where(same, wts_ref[k : k + 1, :], weight)
        mask = mask.astype(BF16)
        sel_v[rows(block), :] = mask
        return mask, jnp.sum(weight, axis=1, keepdims=True)

    pl.semaphore_wait(barrier, n - 1 + 2)

    def build(i, carry):
        mask, weight = select(to(i))
        sent_v[rows(to(i)), :] = (weight * mm(mask, gathered(cot_ref, q))).astype(BF16)
        c_out(i).start()

        @pl.when(jnp.logical_not(across_at(i)))
        def _():
            pair_v[rows(to(i)), :] = (weight * mm(mask, gathered(cot_ref, qy))).astype(BF16)
            c_pair(i).start()

        return carry

    build(2, 0)
    build(1, 0)
    build(3, 0)
    mask, weight = select(me)
    for part in range(tp):
        routed_v[part, rows(me), :] = (weight * mm(mask, gathered(cot_ref, part))).astype(BF16)

    for load in loads:
        load.wait()

    chunk = min(slots, 256)

    def ahead(some):
        pre_g[some, :] = mm(x_v[some, :], wg_v[...])
        pre_u[some, :] = mm(x_v[some, :], wu_v[...])

    def forward(i, carry):
        ahead(pl.ds(pl.multiple_of(i * chunk, chunk), chunk))
        return carry

    def stage_experts(j):
        block = rows(source(j))
        total = mm(routed_v[0, block, :], gathered(wd_v, 0), NT)
        for part in range(1, tp):
            total = total + mm(routed_v[part, block, :], gathered(wd_v, part), NT)
        gate = pre_g[block, :]
        up = pre_u[block, :]
        sig = jax.nn.sigmoid(gate)
        swish = gate * sig
        hid_v[block, :] = (swish * up).astype(BF16)
        g_gate = (total * up * sig * (1.0 + gate * (1.0 - sig))).astype(BF16)
        g_up = (total * swish).astype(BF16)
        gpg_v[block, :] = g_gate
        gpu_v[block, :] = g_up
        for u in range(2 * tp):
            some = slice(u * du, (u + 1) * du)
            part_v[u % tp, block, u // tp * du : (u // tp + 1) * du] = (
                mm(g_gate, wg_v[some, :], NT) + mm(g_up, wu_v[some, :], NT)
            ).astype(BF16)
        c_core(j, 1).start()
        c_core(j, 0).start()

    def share(j):
        c_out(j).wait_recv()
        c_agd(j).start()

        @pl.when(across_at(j))
        def _():
            c_agy(j).start()

    def pass_on(j):
        @pl.when(across_at(j))
        def _():
            c_agy(j).wait_recv()

        @pl.when(jnp.logical_not(across_at(j)))
        def _():
            c_pair(j).wait_recv()

        c_fwd(j).start()

    def stage_cores(j):
        block = rows(source(j))
        c_core(j, 1).wait_recv()
        ysend_v[block, :] = (
            part_v[qy, block, :].astype(F32) + core_v[1, block, :].astype(F32)
        ).astype(BF16)
        c_y(j).start()

    def stage_return(j):
        block = rows(source(j))
        c_core(j, 0).wait_recv()
        c_y(j).wait_recv()
        total = (
            part_v[q, block, :].astype(F32)
            + core_v[0, block, :].astype(F32)
            + yrecv_v[block, :].astype(F32)
        ).astype(BF16)

        @pl.when(j == 0)
        def _():
            ret_v[block, :] = total

        @pl.when(j > 0)
        def _():
            back_v[block, :] = total
            c_ret(j).start()

    def several(block, count):
        return block.at[pl.ds(0, count * cap)]

    def experts(j):
        both = several(sent_v, 2)
        remote(both, both, agd_s, core_in.at[j], me, qd).wait_recv()
        stage_experts(j)

    def pipeline(t, carry):
        @pl.when(t < 4)
        def _():
            share(t + 1)

        @pl.when(t < n - 4)
        def _():
            build(t + 4, 0)

        experts(t)

        stage_cores(t)

        stage_return(t - 1)

        @pl.when(t == 3)
        def _():
            share(t + 2)

        @pl.when(jnp.logical_and(t >= 3, t < n - 3))
        def _():
            share(t + 3)

        @pl.when(t < n - 1)
        def _():
            pass_on(t + 1)

        return carry

    ahead(rows(me))
    stage_experts(0)
    build(4, 0)
    lax.fori_loop(0, slots // chunk // 2, forward, 0)
    stage_cores(0)
    share(1)
    lax.fori_loop(slots // chunk // 2, slots // chunk, forward, 0)
    pass_on(1)
    lax.fori_loop(1, n, pipeline, 0)

    for part in range(tp):
        both = mm(hid_v[...], routed_v[part], TN).astype(BF16)
        gd_out[0, :, part * du : (part + 1) * du] = both[:, :du]
        gd_out[0, :, (part + tp) * du : (part + tp + 1) * du] = both[:, du:]
    piece = min(width, 512)

    def weights(i, carry):
        some = pl.ds(pl.multiple_of(i * piece, piece), piece)
        flipped = x_v[:, some]
        gg_out[0, some, :] = mm(flipped, gpg_v[...], TN).astype(BF16)
        gu_out[0, some, :] = mm(flipped, gpu_v[...], TN).astype(BF16)
        return carry

    lax.fori_loop(0, width // piece // 2, weights, 0)
    stage_return(n - 1)
    lax.fori_loop(width // piece // 2, width // piece, weights, 0)

    back = several(back_v, n - 1)
    remote(back, back, ret_s, ret_r, me, qd).wait_recv()

    def half_of(part, h):
        return mid_v.at[part, :, h * du : (h + 1) * du]

    def passed(part, h, k, there):
        return remote(half_of(part, h), half_of(part, h), mid_s, mid_r.at[2 * k + h], me, there)

    mid_y = [passed(q, h, 0, qy) for h in (0, 1)]
    mid_d = [passed(q, h, 1, qd) for h in (0, 1)]
    mid_f = [passed(qy, h, 2, qd) for h in (0, 1)]
    for h in (0, 1):
        come = mm(sel_v[...], ret_v[:, h * du : (h + 1) * du], TN)
        mid_v[q, :, h * du : (h + 1) * du] = (cot_ref[:, unit(q, h)].astype(F32) + come).astype(BF16)
        mid_y[h].start()
        mid_d[h].start()

    for load in late_loads:
        load.wait()
    gate_in = gin_ref[...].astype(F32)
    conv_sum = csum_ref[...].astype(F32)
    mixed = (gate_in * conv_sum).astype(BF16)
    own_rows = width // n
    owners = n // (2 * tp)

    def owned(block):
        return pl.ds(pl.multiple_of(block * own_rows, own_rows), own_rows)

    def c_term(block, slot):
        return remote(
            term_v.at[owned(block)], terms_v.at[slot], term_s, term_r, block, q
        )

    def send_terms(part, h):
        some = unit(part, h)
        term_v[some, :] = mm(mid_v[part, :, h * du : (h + 1) * du], mixed, TN).astype(BF16)

        def send(i, carry):
            block = (part + h * tp) * owners + i

            @pl.when(block != me)
            def _():
                c_term(block, me).start()

            return carry

        lax.fori_loop(0, owners, send, 0)

    send_terms(q, 0)
    send_terms(q, 1)
    for h in (0, 1):
        mid_d[h].wait_recv()
        send_terms(qd, h)
    mid_y[0].wait_recv()
    mid_f[0].start()
    send_terms(qy, 0)
    mid_f[0].wait_recv()
    send_terms(qdy, 0)
    mid_y[1].wait_recv()
    mid_f[1].start()
    send_terms(qy, 1)
    mid_f[1].wait_recv()
    grad_mixed = jnp.zeros((tokens, mixed.shape[1]), F32)
    for u in range(2 * tp):
        grad_mixed = grad_mixed + mm(
            mid_v[u % tp, :, u // tp * du : (u // tp + 1) * du], ow_ref[u * du : (u + 1) * du, :]
        )
    ext_v[:tokens, :] = grad_mixed * gate_in
    edge = halo_v.shape[0]
    halo = remote(ext_v.at[pl.ds(0, edge)], halo_v, halo_s, halo_r, (me - 1 + n) % n, q)
    halo.start()
    send_terms(qdy, 1)
    for i in range(2):
        own = 2 * q + i
        gi_out[:, i * du : (i + 1) * du] = mid_v[
            own % tp, :, pl.ds(pl.multiple_of(own // tp * du, du), du)
        ]
    ggi_out[...] = (grad_mixed * conv_sum).astype(BF16)

    halo.wait_recv()
    ext_v[tokens:, :] = jnp.where(me == n - 1, 0.0, halo_v[...])
    taps = taps_ref[...]
    grad_prod = (
        taps[0:1, :] * ext_v[2 : tokens + 2, :]
        + taps[1:2, :] * ext_v[1 : tokens + 1, :]
        + taps[2:3, :] * ext_v[:tokens, :]
    )
    gcc_out[...] = (grad_prod * cv_ref[...].astype(F32)).astype(BF16)
    gcv_out[...] = (grad_prod * cc_ref[...].astype(F32)).astype(BF16)

    parts = terms_v.at[pl.ds(0, n - 1)]
    remote(parts, parts, term_s, term_r, me, qd).wait_recv()

    def add_term(i, total):
        return total + terms_v[(me + i) % n].astype(F32)

    gow_out[...] = lax.fori_loop(1, n, add_term, term_v[owned(me), :].astype(F32))

    for sem, block, count in (
        (out_s, sent_v, n - 1),
        (pair_s, sent_v, half - 1),
        (agy_s, sent_v, half),
        (agd_s, sent_v, n - 1),
        (fwd_s, sent_v, n - 1),
        (y_s, sent_v, n),
        (ret_s, sent_v, n - 1),
    ):
        some = several(block, count)
        remote(some, some, sem, halo_r, me, qd).wait_send()
    remote(core_v, core_v, core_s, halo_r, me, qd).wait_send()
    remote(parts, parts, term_s, term_r, me, qd).wait_send()
    thrice = mid_v.at[pl.ds(0, 3)]
    remote(thrice, thrice, mid_s, halo_r, me, qd).wait_send()
    halo.wait_send()


def move(*refs):
    count = (len(refs) - 1) // 2
    outs = [
        pltpu.make_async_copy(refs[i], refs[count + i], refs[-1].at[i]) for i in range(count)
    ]
    for copy in outs:
        copy.start()
    for copy in outs:
        copy.wait()


def moved(arrays):
    count = len(arrays)
    return pl.pallas_call(
        move,
        out_shape=tuple(jax.ShapeDtypeStruct(a.shape, a.dtype) for a in arrays),
        in_specs=[pl.BlockSpec(memory_space=pltpu.VMEM)] * count,
        out_specs=(pl.BlockSpec(memory_space=pl.ANY),) * count,
        scratch_shapes=[pltpu.SemaphoreType.DMA((count,))],
        compiler_params=pltpu.CompilerParams(vmem_limit_bytes=16000 * 1024),
    )(*arrays)


def body(
    cotangent,
    route_ids,
    route_weights,
    expert_inputs,
    gate_weight,
    up_weight,
    down_weight,
    out_weight,
    gate_in,
    conv_sum,
    conv_c,
    conv_v,
    conv_taps,
):
    n = lax.axis_size("sp")
    tp = lax.axis_size("tp")
    tokens, width = cotangent.shape
    slots = expert_inputs.shape[1]
    hidden = gate_weight.shape[2]
    chans = gate_in.shape[1]
    top = route_ids.shape[1]
    dq = width // tp
    vmem = pl.BlockSpec(memory_space=pltpu.VMEM)
    hbm = pl.BlockSpec(memory_space=pl.ANY)
    dma = pltpu.SemaphoreType.DMA
    results = pl.pallas_call(
        functools.partial(kernel, n, tp),
        out_shape=(
            pltpu.VMEM((tokens, dq), BF16),
            pltpu.VMEM(gate_weight.shape, BF16),
            pltpu.VMEM(up_weight.shape, BF16),
            pltpu.VMEM(down_weight.shape, BF16),
            pltpu.VMEM((width // n, chans), F32),
            pltpu.VMEM((tokens, chans), BF16),
            pltpu.VMEM((tokens, chans), BF16),
            pltpu.VMEM((tokens, chans), BF16),
        ),
        in_specs=[hbm] * 13,
        out_specs=(vmem,) * 8,
        scratch_shapes=[
            pltpu.VMEM((top, tokens), jnp.int32),
            pltpu.VMEM((top, tokens), F32),
            pltpu.VMEM((tokens, width), BF16),
            pltpu.VMEM((width, chans), BF16),
            pltpu.VMEM((tokens, chans), BF16),
            pltpu.VMEM((tokens, chans), BF16),
            pltpu.VMEM((tokens, chans), BF16),
            pltpu.VMEM((tokens, chans), BF16),
            pltpu.VMEM(conv_taps.shape, F32),
            pltpu.VMEM((slots, width), BF16),
            pltpu.VMEM((width, hidden), BF16),
            pltpu.VMEM((width, hidden), BF16),
            pltpu.VMEM((hidden, width), BF16),
            pltpu.VMEM((slots, tokens), BF16),
            pltpu.VMEM((slots, dq), BF16),
            pltpu.VMEM((slots, dq), BF16),
            pltpu.VMEM((tp, slots, dq), BF16),
            pltpu.VMEM((slots, hidden), F32),
            pltpu.VMEM((slots, hidden), F32),
            pltpu.VMEM((slots, hidden), BF16),
            pltpu.VMEM((slots, hidden), BF16),
            pltpu.VMEM((slots, hidden), BF16),
            pltpu.VMEM((tp, slots, dq), BF16),
            pltpu.VMEM((2, slots, dq), BF16),
            pltpu.VMEM((slots, dq), BF16),
            pltpu.VMEM((slots, dq), BF16),
            pltpu.VMEM((slots, dq), BF16),
            pltpu.VMEM((slots, dq), BF16),
            pltpu.VMEM((tp, tokens, dq), BF16),
            pltpu.VMEM((width, chans), BF16),
            pltpu.VMEM((n, width // n, chans), BF16),
            pltpu.VMEM((tokens + 8, chans), F32),
            pltpu.VMEM((8, chans), F32),
            dma((4,)),
            dma((9,)),
        ]
        + [dma(())] * 11
        + [
            dma((n,)),
            dma((n,)),
            dma((n,)),
            dma((2, n)),
            dma((n,)),
            dma(()),
            dma(()),
            dma((6,)),
            dma(()),
        ],
        compiler_params=pltpu.CompilerParams(
            collective_id=0, has_side_effects=True, vmem_limit_bytes=61696 * 1024
        ),
    )(
        route_ids.T,
        route_weights.T,
        cotangent,
        expert_inputs,
        gate_weight,
        up_weight,
        down_weight,
        out_weight,
        gate_in,
        conv_sum,
        conv_c,
        conv_v,
        conv_taps,
    )
    return moved(results)


def solution(mesh):
    placed = (
        P("sp", None),
        P("sp", None),
        P("sp", None),
        P("sp", None, None),
        P("sp", None, "tp"),
        P("sp", None, "tp"),
        P("sp", "tp", None),
        P(None, "tp"),
        P("sp", "tp"),
        P("sp", "tp"),
        P("sp", "tp"),
        P("sp", "tp"),
        P(None, "tp"),
    )
    return jax.shard_map(
        body,
        mesh=mesh,
        in_specs=placed,
        out_specs=(
            P("sp", "tp"),
            P("sp", None, "tp"),
            P("sp", None, "tp"),
            P("sp", "tp", None),
            P("sp", "tp"),
            P("sp", "tp"),
            P("sp", "tp"),
            P("sp", "tp"),
        ),
        check_vma=False,
    )
```

```python
import functools

import jax
import jax.numpy as jnp
from jax import lax
from jax.experimental import pallas as pl
from jax.experimental.pallas import tpu as pltpu
from jax.sharding import PartitionSpec as P

F32 = jnp.float32
BF16 = jnp.bfloat16
NT = (((1,), (1,)), ((), ()))
TN = (((0,), (0,)), ((), ()))


def mm(a, b, dims=(((1,), (0,)), ((), ()))):
    return lax.dot_general(a, b, dims, preferred_element_type=F32)


def kernel(
    n,
    tp,
    ids_hbm,
    wts_hbm,
    cot_hbm,
    x_hbm,
    wg_hbm,
    wu_hbm,
    wd_hbm,
    ow_hbm,
    gin_hbm,
    csum_hbm,
    cc_hbm,
    cv_hbm,
    taps_hbm,
    gi_out,
    gg_out,
    gu_out,
    gd_out,
    gow_out,
    ggi_out,
    gcc_out,
    gcv_out,
    ids_ref,
    wts_ref,
    cot_ref,
    ow_ref,
    gin_ref,
    csum_ref,
    cc_ref,
    cv_ref,
    taps_ref,
    x_v,
    wg_v,
    wu_v,
    wd_v,
    sel_v,
    sent_v,
    pair_v,
    routed_v,
    pre_g,
    pre_u,
    hid_v,
    gpg_v,
    gpu_v,
    part_v,
    core_v,
    ysend_v,
    yrecv_v,
    back_v,
    ret_v,
    mid_v,
    term_v,
    terms_v,
    ext_v,
    halo_v,
    load_sem,
    side_sem,
    out_s,
    pair_s,
    agy_s,
    agd_s,
    fwd_s,
    core_s,
    y_s,
    ret_s,
    term_s,
    mid_s,
    halo_s,
    out_r,
    agy_r,
    core_in,
    core_r,
    y_r,
    ret_r,
    term_r,
    mid_r,
    halo_r,
):
    me = lax.axis_index("sp")
    q = lax.axis_index("tp")
    qd = q + 1 - 2 * (q % 2)
    qy = (q + tp // 2) % tp
    qdy = (qd + tp // 2) % tp
    tokens, width = cot_ref.shape
    slots = x_v.shape[0]
    cap = slots // n
    dq = width // tp
    du = dq // 2
    top = ids_ref.shape[0]

    barrier = pltpu.get_barrier_semaphore()

    def greet(i, carry):
        pl.semaphore_signal(
            barrier, inc=1, device_id=((me + i) % n, q), device_id_type=pl.DeviceIdType.MESH
        )
        return carry

    lax.fori_loop(1, n, greet, 0)
    for other in (qd, qy):
        pl.semaphore_signal(
            barrier, inc=1, device_id=(me, other), device_id_type=pl.DeviceIdType.MESH
        )

    first_loads = [
        pltpu.make_async_copy(src, dst, side_sem.at[i])
        for i, (src, dst) in enumerate(
            ((ids_hbm, ids_ref), (wts_hbm, wts_ref), (cot_hbm, cot_ref))
        )
    ]
    loads = [
        pltpu.make_async_copy(src.at[0], dst, load_sem.at[i])
        for i, (src, dst) in enumerate(
            ((wg_hbm, wg_v), (wu_hbm, wu_v), (wd_hbm, wd_v), (x_hbm, x_v))
        )
    ]
    late_loads = [
        pltpu.make_async_copy(src, dst, side_sem.at[i + 3])
        for i, (src, dst) in enumerate(
            (
                (ow_hbm, ow_ref),
                (gin_hbm, gin_ref),
                (csum_hbm, csum_ref),
                (cc_hbm, cc_ref),
                (cv_hbm, cv_ref),
                (taps_hbm, taps_ref),
            )
        )
    ]

    for load in (*first_loads, *loads, *late_loads):
        load.start()

    def rows(block):
        return pl.ds(pl.multiple_of(block * cap, cap), cap)

    def unit(part, side):
        return pl.ds(pl.multiple_of((part + side * tp) * du, du), du)

    def gathered(ref, part):
        return jnp.concatenate([ref[:, unit(part, 0)], ref[:, unit(part, 1)]], axis=1)

    def remote(src, dst, ssem, rsem, sp_id, tp_id):
        return pltpu.make_async_remote_copy(
            src_ref=src,
            dst_ref=dst,
            send_sem=ssem,
            recv_sem=rsem,
            device_id=(sp_id, tp_id),
            device_id_type=pl.DeviceIdType.MESH,
        )

    half = n // 2
    pairs = half // 2
    side, low = me // half, me % half
    pair, member = low // 2, low % 2

    def index(p):
        swapped = jnp.where((p == half + 1) | (p == half + 2), 2 * half - p, p - 3)
        far = half + jnp.where(p == 2, 0, swapped)
        near = jnp.where(p < 2, p, jnp.where(p == 3, 2, p - half))
        return jnp.where((p == 2) | ((p > 3) & (p < half + 3)), far, near)

    def across_at(p):
        return index(p) >= half

    def step(p):
        i = index(p)
        across = jnp.where(i >= half, 1, 0)
        turn = i % half
        return (side + across) % 2 * half, turn // 2, turn % 2

    def to(i):
        base, hop, swap = step(i)
        return base + (pair + hop) % pairs * 2 + (member + swap) % 2

    def source(i):
        base, hop, swap = step(i)
        return base + (pair - hop + pairs) % pairs * 2 + (member + swap) % 2

    def c_out(i):
        return remote(
            sent_v.at[rows(to(i))], routed_v.at[q, rows(me)], out_s, out_r.at[i], to(i), q
        )

    def c_pair(i):
        return remote(
            pair_v.at[rows(to(i))],
            routed_v.at[qy, rows(me)],
            pair_s,
            agy_r.at[i],
            to(i),
            q,
        )

    def c_agy(i):
        block = routed_v.at[q, rows(source(i))]
        return remote(block, block, agy_s, agy_r.at[i], me, qy)

    def c_agd(i):
        block = routed_v.at[q, rows(source(i))]
        return remote(block, block, agd_s, core_in.at[i], me, qd)

    def c_fwd(i):
        block = routed_v.at[qy, rows(source(i))]
        return remote(block, block, fwd_s, core_in.at[i], me, qd)

    def c_core(i, h):
        return remote(
            part_v.at[(qd, qdy)[h], rows(source(i))],
            core_v.at[h, rows(source(i))],
            core_s,
            core_r.at[h, i],
            me,
            qd,
        )

    def c_y(i):
        block = rows(source(i))
        return remote(ysend_v.at[block], yrecv_v.at[block], y_s, y_r.at[i], me, qy)

    def c_ret(i):
        return remote(
            back_v.at[rows(source(i))], ret_v.at[rows(me)], ret_s, ret_r, source(i), q
        )

    for load in first_loads:
        load.wait()
    ids = ids_ref[...]
    experts = n
    e_iota = lax.broadcasted_iota(jnp.int32, (experts, tokens), 0)
    hits = [e_iota == ids[k : k + 1, :] for k in range(top)]
    named = hits[0].astype(F32)
    for k in range(1, top):
        named = named + hits[k].astype(F32)
    earlier = (
        lax.broadcasted_iota(jnp.int32, (tokens, tokens), 0)
        < lax.broadcasted_iota(jnp.int32, (tokens, tokens), 1)
    ).astype(F32).astype(BF16)
    before = mm(named.astype(BF16), earlier)
    place = [
        jnp.sum(jnp.where(hits[k], before, 0.0), axis=0, keepdims=True)
        + ids[k : k + 1, :].astype(F32) * cap
        for k in range(top)
    ]
    slot_iota = lax.broadcasted_iota(jnp.int32, (cap, tokens), 0)

    def select(block):
        slot = (slot_iota + block * cap).astype(F32)
        mask = jnp.zeros((cap, tokens), F32)
        weight = jnp.zeros((cap, tokens), F32)
        for k in range(top):
            same = slot == place[k]
            mask = jnp.where(same, 1.0, mask)
            weight = jnp.where(same, wts_ref[k : k + 1, :], weight)
        mask = mask.astype(BF16)
        sel_v[rows(block), :] = mask
        return mask, jnp.sum(weight, axis=1, keepdims=True)

    pl.semaphore_wait(barrier, n - 1 + 2)

    def build(i, carry):
        mask, weight = select(to(i))
        sent_v[rows(to(i)), :] = (weight * mm(mask, gathered(cot_ref, q))).astype(BF16)
        c_out(i).start()

        @pl.when(jnp.logical_not(across_at(i)))
        def _():
            pair_v[rows(to(i)), :] = (weight * mm(mask, gathered(cot_ref, qy))).astype(BF16)
            c_pair(i).start()

        return carry

    build(2, 0)
    build(1, 0)
    build(3, 0)
    mask, weight = select(me)
    for part in range(tp):
        routed_v[part, rows(me), :] = (weight * mm(mask, gathered(cot_ref, part))).astype(BF16)

    for load in loads:
        load.wait()

    chunk = min(slots, 256)

    def ahead(some):
        pre_g[some, :] = mm(x_v[some, :], wg_v[...])
        pre_u[some, :] = mm(x_v[some, :], wu_v[...])

    def forward(i, carry):
        ahead(pl.ds(pl.multiple_of(i * chunk, chunk), chunk))
        return carry

    def stage_experts(j):
        block = rows(source(j))
        total = mm(routed_v[0, block, :], gathered(wd_v, 0), NT)
        for part in range(1, tp):
            total = total + mm(routed_v[part, block, :], gathered(wd_v, part), NT)
        gate = pre_g[block, :]
        up = pre_u[block, :]
        sig = jax.nn.sigmoid(gate)
        swish = gate * sig
        hid_v[block, :] = (swish * up).astype(BF16)
        g_gate = (total * up * sig * (1.0 + gate * (1.0 - sig))).astype(BF16)
        g_up = (total * swish).astype(BF16)
        gpg_v[block, :] = g_gate
        gpu_v[block, :] = g_up
        for u in range(2 * tp):
            some = slice(u * du, (u + 1) * du)
            part_v[u % tp, block, u // tp * du : (u // tp + 1) * du] = (
                mm(g_gate, wg_v[some, :], NT) + mm(g_up, wu_v[some, :], NT)
            ).astype(BF16)
        c_core(j, 1).start()
        c_core(j, 0).start()

    def share(j):
        c_out(j).wait_recv()
        c_agd(j).start()

        @pl.when(across_at(j))
        def _():
            c_agy(j).start()

    def pass_on(j):
        @pl.when(across_at(j))
        def _():
            c_agy(j).wait_recv()

        @pl.when(jnp.logical_not(across_at(j)))
        def _():
            c_pair(j).wait_recv()

        c_fwd(j).start()

    def stage_cores(j):
        block = rows(source(j))
        c_core(j, 1).wait_recv()
        ysend_v[block, :] = (
            part_v[qy, block, :].astype(F32) + core_v[1, block, :].astype(F32)
        ).astype(BF16)
        c_y(j).start()

    def stage_return(j):
        block = rows(source(j))
        c_core(j, 0).wait_recv()
        c_y(j).wait_recv()
        total = (
            part_v[q, block, :].astype(F32)
            + core_v[0, block, :].astype(F32)
            + yrecv_v[block, :].astype(F32)
        ).astype(BF16)

        @pl.when(j == 0)
        def _():
            ret_v[block, :] = total

        @pl.when(j > 0)
        def _():
            back_v[block, :] = total
            c_ret(j).start()

    def several(block, count):
        return block.at[pl.ds(0, count * cap)]

    def experts(j):
        both = several(sent_v, 2)
        remote(both, both, agd_s, core_in.at[j], me, qd).wait_recv()
        stage_experts(j)

    def pipeline(t, carry):
        @pl.when(t < 4)
        def _():
            share(t + 1)

        @pl.when(t < n - 4)
        def _():
            build(t + 4, 0)

        experts(t)

        @pl.when(t != 3)
        def _():
            stage_cores(t)

        @pl.when(t == 6)
        def _():
            stage_cores(3)

        @pl.when(t != 4)
        def _():
            stage_return(t - 1)

        @pl.when(t == 7)
        def _():
            stage_return(3)

        @pl.when(t == 3)
        def _():
            share(t + 2)

        @pl.when(jnp.logical_and(t > 3, t < n - 3))
        def _():
            share(t + 3)

        @pl.when(t < n - 1)
        def _():
            pass_on(t + 1)

        @pl.when(t == 3)
        def _():
            share(t + 3)

        return carry

    ahead(rows(me))
    stage_experts(0)
    build(4, 0)
    lax.fori_loop(0, slots // chunk // 2, forward, 0)
    stage_cores(0)
    share(1)
    lax.fori_loop(slots // chunk // 2, slots // chunk, forward, 0)
    pass_on(1)
    lax.fori_loop(1, n, pipeline, 0)

    for part in range(tp):
        both = mm(hid_v[...], routed_v[part], TN).astype(BF16)
        gd_out[0, :, part * du : (part + 1) * du] = both[:, :du]
        gd_out[0, :, (part + tp) * du : (part + tp + 1) * du] = both[:, du:]
    piece = min(width, 512)

    def weights(i, carry):
        some = pl.ds(pl.multiple_of(i * piece, piece), piece)
        flipped = x_v[:, some]
        gg_out[0, some, :] = mm(flipped, gpg_v[...], TN).astype(BF16)
        gu_out[0, some, :] = mm(flipped, gpu_v[...], TN).astype(BF16)
        return carry

    lax.fori_loop(0, width // piece // 2, weights, 0)
    stage_return(n - 1)
    lax.fori_loop(width // piece // 2, width // piece, weights, 0)

    back = several(back_v, n - 1)
    remote(back, back, ret_s, ret_r, me, qd).wait_recv()

    def half_of(part, h):
        return mid_v.at[part, :, h * du : (h + 1) * du]

    def passed(part, h, k, there):
        return remote(half_of(part, h), half_of(part, h), mid_s, mid_r.at[2 * k + h], me, there)

    mid_y = [passed(q, h, 0, qy) for h in (0, 1)]
    mid_d = [passed(q, h, 1, qd) for h in (0, 1)]
    mid_f = [passed(qy, h, 2, qd) for h in (0, 1)]
    for h in (0, 1):
        come = mm(sel_v[...], ret_v[:, h * du : (h + 1) * du], TN)
        mid_v[q, :, h * du : (h + 1) * du] = (cot_ref[:, unit(q, h)].astype(F32) + come).astype(BF16)
        mid_y[h].start()
        mid_d[h].start()

    for load in late_loads:
        load.wait()
    gate_in = gin_ref[...].astype(F32)
    conv_sum = csum_ref[...].astype(F32)
    mixed = (gate_in * conv_sum).astype(BF16)
    own_rows = width // n
    owners = n // (2 * tp)

    def owned(block):
        return pl.ds(pl.multiple_of(block * own_rows, own_rows), own_rows)

    def c_term(block, slot):
        return remote(
            term_v.at[owned(block)], terms_v.at[slot], term_s, term_r, block, q
        )

    def send_terms(part, h):
        some = unit(part, h)
        term_v[some, :] = mm(mid_v[part, :, h * du : (h + 1) * du], mixed, TN).astype(BF16)

        def send(i, carry):
            block = (part + h * tp) * owners + i

            @pl.when(block != me)
            def _():
                c_term(block, me).start()

            return carry

        lax.fori_loop(0, owners, send, 0)

    send_terms(q, 0)
    send_terms(q, 1)
    for h in (0, 1):
        mid_d[h].wait_recv()
        send_terms(qd, h)
    mid_y[0].wait_recv()
    mid_f[0].start()
    send_terms(qy, 0)
    mid_f[0].wait_recv()
    send_terms(qdy, 0)
    mid_y[1].wait_recv()
    mid_f[1].start()
    send_terms(qy, 1)
    mid_f[1].wait_recv()
    grad_mixed = jnp.zeros((tokens, mixed.shape[1]), F32)
    for u in range(2 * tp):
        grad_mixed = grad_mixed + mm(
            mid_v[u % tp, :, u // tp * du : (u // tp + 1) * du], ow_ref[u * du : (u + 1) * du, :]
        )
    ext_v[:tokens, :] = grad_mixed * gate_in
    edge = halo_v.shape[0]
    halo = remote(ext_v.at[pl.ds(0, edge)], halo_v, halo_s, halo_r, (me - 1 + n) % n, q)
    halo.start()
    send_terms(qdy, 1)
    for i in range(2):
        own = 2 * q + i
        gi_out[:, i * du : (i + 1) * du] = mid_v[
            own % tp, :, pl.ds(pl.multiple_of(own // tp * du, du), du)
        ]
    ggi_out[...] = (grad_mixed * conv_sum).astype(BF16)

    halo.wait_recv()
    ext_v[tokens:, :] = jnp.where(me == n - 1, 0.0, halo_v[...])
    taps = taps_ref[...]
    grad_prod = (
        taps[0:1, :] * ext_v[2 : tokens + 2, :]
        + taps[1:2, :] * ext_v[1 : tokens + 1, :]
        + taps[2:3, :] * ext_v[:tokens, :]
    )
    gcc_out[...] = (grad_prod * cv_ref[...].astype(F32)).astype(BF16)
    gcv_out[...] = (grad_prod * cc_ref[...].astype(F32)).astype(BF16)

    parts = terms_v.at[pl.ds(0, n - 1)]
    remote(parts, parts, term_s, term_r, me, qd).wait_recv()

    def add_term(i, total):
        return total + terms_v[(me + i) % n].astype(F32)

    gow_out[...] = lax.fori_loop(1, n, add_term, term_v[owned(me), :].astype(F32))

    for sem, block, count in (
        (out_s, sent_v, n - 1),
        (pair_s, sent_v, half - 1),
        (agy_s, sent_v, half),
        (agd_s, sent_v, n - 1),
        (fwd_s, sent_v, n - 1),
        (y_s, sent_v, n),
        (ret_s, sent_v, n - 1),
    ):
        some = several(block, count)
        remote(some, some, sem, halo_r, me, qd).wait_send()
    remote(core_v, core_v, core_s, halo_r, me, qd).wait_send()
    remote(parts, parts, term_s, term_r, me, qd).wait_send()
    thrice = mid_v.at[pl.ds(0, 3)]
    remote(thrice, thrice, mid_s, halo_r, me, qd).wait_send()
    halo.wait_send()


def move(*refs):
    count = (len(refs) - 1) // 2
    outs = [
        pltpu.make_async_copy(refs[i], refs[count + i], refs[-1].at[i]) for i in range(count)
    ]
    for copy in outs:
        copy.start()
    for copy in outs:
        copy.wait()


def moved(arrays):
    count = len(arrays)
    return pl.pallas_call(
        move,
        out_shape=tuple(jax.ShapeDtypeStruct(a.shape, a.dtype) for a in arrays),
        in_specs=[pl.BlockSpec(memory_space=pltpu.VMEM)] * count,
        out_specs=(pl.BlockSpec(memory_space=pl.ANY),) * count,
        scratch_shapes=[pltpu.SemaphoreType.DMA((count,))],
        compiler_params=pltpu.CompilerParams(vmem_limit_bytes=16000 * 1024),
    )(*arrays)


def body(
    cotangent,
    route_ids,
    route_weights,
    expert_inputs,
    gate_weight,
    up_weight,
    down_weight,
    out_weight,
    gate_in,
    conv_sum,
    conv_c,
    conv_v,
    conv_taps,
):
    n = lax.axis_size("sp")
    tp = lax.axis_size("tp")
    tokens, width = cotangent.shape
    slots = expert_inputs.shape[1]
    hidden = gate_weight.shape[2]
    chans = gate_in.shape[1]
    top = route_ids.shape[1]
    dq = width // tp
    vmem = pl.BlockSpec(memory_space=pltpu.VMEM)
    hbm = pl.BlockSpec(memory_space=pl.ANY)
    dma = pltpu.SemaphoreType.DMA
    results = pl.pallas_call(
        functools.partial(kernel, n, tp),
        out_shape=(
            pltpu.VMEM((tokens, dq), BF16),
            pltpu.VMEM(gate_weight.shape, BF16),
            pltpu.VMEM(up_weight.shape, BF16),
            pltpu.VMEM(down_weight.shape, BF16),
            pltpu.VMEM((width // n, chans), F32),
            pltpu.VMEM((tokens, chans), BF16),
            pltpu.VMEM((tokens, chans), BF16),
            pltpu.VMEM((tokens, chans), BF16),
        ),
        in_specs=[hbm] * 13,
        out_specs=(vmem,) * 8,
        scratch_shapes=[
            pltpu.VMEM((top, tokens), jnp.int32),
            pltpu.VMEM((top, tokens), F32),
            pltpu.VMEM((tokens, width), BF16),
            pltpu.VMEM((width, chans), BF16),
            pltpu.VMEM((tokens, chans), BF16),
            pltpu.VMEM((tokens, chans), BF16),
            pltpu.VMEM((tokens, chans), BF16),
            pltpu.VMEM((tokens, chans), BF16),
            pltpu.VMEM(conv_taps.shape, F32),
            pltpu.VMEM((slots, width), BF16),
            pltpu.VMEM((width, hidden), BF16),
            pltpu.VMEM((width, hidden), BF16),
            pltpu.VMEM((hidden, width), BF16),
            pltpu.VMEM((slots, tokens), BF16),
            pltpu.VMEM((slots, dq), BF16),
            pltpu.VMEM((slots, dq), BF16),
            pltpu.VMEM((tp, slots, dq), BF16),
            pltpu.VMEM((slots, hidden), F32),
            pltpu.VMEM((slots, hidden), F32),
            pltpu.VMEM((slots, hidden), BF16),
            pltpu.VMEM((slots, hidden), BF16),
            pltpu.VMEM((slots, hidden), BF16),
            pltpu.VMEM((tp, slots, dq), BF16),
            pltpu.VMEM((2, slots, dq), BF16),
            pltpu.VMEM((slots, dq), BF16),
            pltpu.VMEM((slots, dq), BF16),
            pltpu.VMEM((slots, dq), BF16),
            pltpu.VMEM((slots, dq), BF16),
            pltpu.VMEM((tp, tokens, dq), BF16),
            pltpu.VMEM((width, chans), BF16),
            pltpu.VMEM((n, width // n, chans), BF16),
            pltpu.VMEM((tokens + 8, chans), F32),
            pltpu.VMEM((8, chans), F32),
            dma((4,)),
            dma((9,)),
        ]
        + [dma(())] * 11
        + [
            dma((n,)),
            dma((n,)),
            dma((n,)),
            dma((2, n)),
            dma((n,)),
            dma(()),
            dma(()),
            dma((6,)),
            dma(()),
        ],
        compiler_params=pltpu.CompilerParams(
            collective_id=0, has_side_effects=True, vmem_limit_bytes=61696 * 1024
        ),
    )(
        route_ids.T,
        route_weights.T,
        cotangent,
        expert_inputs,
        gate_weight,
        up_weight,
        down_weight,
        out_weight,
        gate_in,
        conv_sum,
        conv_c,
        conv_v,
        conv_taps,
    )
    return moved(results)


def solution(mesh):
    placed = (
        P("sp", None),
        P("sp", None),
        P("sp", None),
        P("sp", None, None),
        P("sp", None, "tp"),
        P("sp", None, "tp"),
        P("sp", "tp", None),
        P(None, "tp"),
        P("sp", "tp"),
        P("sp", "tp"),
        P("sp", "tp"),
        P("sp", "tp"),
        P(None, "tp"),
    )
    return jax.shard_map(
        body,
        mesh=mesh,
        in_specs=placed,
        out_specs=(
            P("sp", "tp"),
            P("sp", None, "tp"),
            P("sp", None, "tp"),
            P("sp", "tp", None),
            P("sp", "tp"),
            P("sp", "tp"),
            P("sp", "tp"),
            P("sp", "tp"),
        ),
        check_vma=False,
    )
```
